32 devices in a mesh: ep: 8 (over z, core), tp: 4 (over y, x).
Axes of the slice: x: 2, y: 2, z: 4, core: 2. Of those that a mesh axis runs over, the one named last changes fastest.
Arguments:
- residual: bfloat16 [512, 2048], P('ep', 'tp')
- state_re: float32 [512, 64, 64], P('ep', 'tp'), may hold values from -4 to 4
- state_im: float32 [512, 64, 64], P('ep', 'tp'), may hold values from -4 to 4
- mix_gain: float32 [2048], replicated, may hold values from 0.1 to 1.9
- proj_in: bfloat16 [2048, 1024], P(None, 'tp'), may hold values from -0.125 to 0.125
- decay_rate: float32 [64, 64], P('tp'), may hold values from 0.1 to 10
- frequency: float32 [64, 64], P('tp'), may hold values from 0 to 201.06177
- log_step: float32 [64], P('tp'), may hold values from -6.9078 to -2.3026
- input_re: float32 [64, 64, 16], P('tp'), may hold values from -1 to 1
- input_im: float32 [64, 64, 16], P('tp'), may hold values from -1 to 1
- read_re: float32 [64, 16, 64], P('tp'), may hold values from -0.5 to 0.5
- read_im: float32 [64, 16, 64], P('tp'), may hold values from -0.5 to 0.5
- skip_gain: float32 [1024], P('tp'), may hold values from -4 to 4
- glu_weight: bfloat16 [1024, 1024], P(None, 'tp'), may hold values from -0.1875 to 0.1875
- out_proj: bfloat16 [1024, 2048], P(None, 'tp'), may hold values from -0.1875 to 0.1875
- ffn_gain: float32 [2048], replicated, may hold values from 0.1 to 1.9
- router: float32 [2048, 8], replicated, may hold values from -0.125 to 0.125
- gate_weight: bfloat16 [8, 2048, 4096], P('ep', None, 'tp'), may hold values from -0.33007812 to 0.33007812
- up_weight: bfloat16 [8, 2048, 4096], P('ep', None, 'tp'), may hold values from -0.33007812 to 0.33007812
- down_weight: bfloat16 [8, 4096, 2048], P('ep', 'tp'), may hold values from -0.046875 to 0.046875
- route_ids: int32 [512, 4], P('ep'), may hold values from 0 to 7, all different within a row; in each aligned block of 64 rows (0 to 63, 64 to 127, ...) at most 33 rows name the same one
Outputs:
- layer_out: bfloat16 [512, 2048], P('ep', 'tp')
- state_re_new: float32 [512, 64, 64], P('ep', 'tp')
- state_im_new: float32 [512, 64, 64], P('ep', 'tp')
The draws below stay inside these ranges and needn't reach their ends.
Inputs may be any that keep to these rules, and one draw needn't show every extreme that they name: `route_ids`: each row names 4 different experts. Within the rows of one ep index (aligned blocks of 64 rows) no expert is named more than 33 times, and in some block some expert is named exactly 33 times.
All inputs are finite; a program needn't handle non-finite values.
Results may differ from the reference program's by a relative error of at most 0.014.
Values may be sent and summed in bfloat16 or wider, within the bound.
A program may use at most 64 MiB of HBM per device.

```python
import math
import jax
import jax.numpy as jnp
import numpy as np
from jax import lax

D = 2048
GROUPS = 64
GROUP_CH = 16
STATE = 64
FF = 4096
TOPK = 4
SEQ_DEV = 64
CH = 1024
EXPERTS = 8
SEQS = 512
CAP = 33
N_EP = 8
N_TP = 4


def draw_residual(key, part):
    key_base = jax.random.fold_in(key, 11)
    key_rows = jax.random.fold_in(key, 12)
    column = jnp.arange(D, dtype=jnp.float32) / D
    row_scale = jnp.exp(jax.random.uniform(key_rows, (SEQS, 1), jnp.float32, math.log(0.3), math.log(3.0)))
    base = jax.random.normal(key_base, (SEQS, D), jnp.float32)
    col_scale = 0.3 * jnp.exp(column * math.log(10.0))
    values = base * row_scale * col_scale[None, :]
    return values.astype(jnp.bfloat16)


def strengthened(array, own_key, source, target, shards_of, factor):
    owner, partner = [(jnp.arange(array.shape[axis_at]) // (array.shape[axis_at] // shards_of)).reshape([-1 if axis == axis_at else 1 for axis in range(array.ndim)]) for axis_at in (source, target)]
    chosen = jax.random.permutation(own_key, shards_of)[partner]
    strong = (owner == chosen) | (owner == (partner + shards_of // 2) % shards_of)
    return jnp.where(strong, factor * array, array)


def block_scale(key, shape, split, smallest, high):
    level, own = 1.0, jax.random.fold_in(key, 6)
    for dim, blocks in split:
        draws = jnp.exp(jax.random.uniform(jax.random.fold_in(own, dim), (blocks,), jnp.float32, smallest / len(split), high / len(split)))
        level = level * jnp.repeat(draws, shape[dim] // blocks).reshape([-1 if axis == dim else 1 for axis in range(len(shape))])
    return level


def assign_block(stream_key, own, number, rows, count, top, limit, skew):
    order = jax.random.permutation(stream_key, count)
    crowded, usual = load_shares(count, rows * top, limit, skew, True), load_shares(count, rows * top, limit, skew, False)
    places = jnp.arange(count)

    def named(sizes, turn):
        used = int((sizes > 0).sum())
        fixed = max(1, used // 4)
        passed = fixed + (places - fixed + turn * (used - fixed)) % max(1, count - fixed)
        return jnp.zeros((count,), jnp.int32).at[order[jnp.where(places < fixed, places, passed)]].set(jnp.asarray(sizes, jnp.int32))

    sizes = jnp.where(number % 4 == 0, named(crowded, number // 4), named(usual, number - number // 4 - 1))
    mixed = jax.random.permutation(jax.random.fold_in(own, 3), count)
    giver, receiver = mixed[0:count // 2 * 2:2], mixed[1:count // 2 * 2:2]
    margin = jnp.minimum(sizes[giver] - 1, limit - sizes[receiver]) // 2
    margin = jnp.where((giver == order[0]) | (receiver == order[0]) | (sizes[receiver] == 0), 0, jnp.maximum(margin, 0))
    passed = jax.random.randint(jax.random.fold_in(own, 4), (count // 2,), 0, 1 << 20) % (margin + 1)
    sizes = sizes.at[giver].add(-passed).at[receiver].add(passed)
    items = jnp.searchsorted(jnp.cumsum(sizes), jnp.arange(rows * top), side="right").astype(jnp.int32)
    listing = items.reshape(top, rows).T
    listing = listing[jax.random.permutation(jax.random.fold_in(own, 1), rows)]
    turn = jax.random.randint(jax.random.fold_in(own, 2), (rows, 1), 0, top)
    return jnp.take_along_axis(listing, (jnp.arange(top)[None, :] + turn) % top, axis=1)


def load_shares(number_of, total, reach, skew, full):
    weights = [(1 << 20) // math.isqrt(rank ** skew) + 1 for rank in range(1, number_of + 1)]
    largest = reach if full else min(reach, max(-(-total // number_of), total * weights[0] // sum(weights)))
    least = 1 if total - largest >= number_of - 1 else 0
    holding, spare = [largest] + [least] * (number_of - 1), total - largest - least * (number_of - 1)
    while spare > 0:
        movable = [i for i in range(1, number_of) if holding[i] < largest] or [i for i in range(1, number_of) if holding[i] < reach]
        mass, left = sum([weights[i] for i in movable]), spare
        for i in movable:
            more = min(reach - holding[i], max(1, left * weights[i] // mass), spare)
            holding[i] = holding[i] + more
            spare = spare - more
    return np.array(holding)


def centred(key, shape, width, reach, cuts=(), held_as=jnp.bfloat16):
    gain = block_scale(key, shape, cuts, -0.22, 0.18) if cuts else 1.0
    entries = jax.random.normal(key, shape, jnp.float32) * width * gain
    return jnp.minimum(jnp.maximum(entries, -reach), reach).astype(held_as)


def heavy_noise(stream_key, shape, scale, bound, split, heavy, held_as=jnp.bfloat16):
    drawn = scale * jax.random.normal(stream_key, shape, jnp.float32)
    if split:
        drawn = drawn * block_scale(stream_key, shape, split, -0.22, 0.18)
    return jnp.clip(strengthened(drawn, jax.random.fold_in(stream_key, 3), *heavy), -bound, bound).astype(held_as)


def setup_inputs(seed: int = 0) -> dict:
    arg_keys = jax.random.split(jax.random.key(seed), 22)
    residual = draw_residual(jax.random.fold_in(arg_keys[21], 71), 0)
    state_re = centred(arg_keys[1], (SEQS, GROUPS, STATE), 0.5, 4.0, ((0, 8), (1, 4)), jnp.float32)
    state_im = centred(arg_keys[2], (SEQS, GROUPS, STATE), 0.5, 4.0, ((0, 8), (1, 4)), jnp.float32)
    mix_gain = jnp.clip(1.0 + 0.18 * jax.random.normal(arg_keys[3], (D,), jnp.float32), 0.1, 1.9)
    proj_in = centred(arg_keys[4], (D, CH), D ** -0.5, 0.125, ((1, 4),))
    decay_rate = jnp.clip(jnp.exp(math.log(10.0) - 4.6051702 * jax.random.uniform(arg_keys[5], (GROUPS, STATE), jnp.float32) ** block_scale(arg_keys[5], (GROUPS, STATE), ((0, 4),), -0.2, 0.2)), 0.1, 10.0)
    frequency = jnp.clip(201.06177 * jax.random.uniform(arg_keys[6], (GROUPS, STATE), jnp.float32) ** block_scale(arg_keys[6], (GROUPS, STATE), ((0, 4),), -0.2, 0.2), 0.0, 201.06177)
    log_step = jnp.clip(-6.9078 + 4.6052003 * jax.random.uniform(arg_keys[7], (GROUPS,), jnp.float32) ** block_scale(arg_keys[7], (GROUPS,), ((0, 4),), -0.2, 0.2), -6.9078, -2.3026)
    input_re = centred(arg_keys[8], (GROUPS, STATE, GROUP_CH), (2 * GROUP_CH) ** -0.5, 1.0, ((0, 4),), jnp.float32)
    input_im = centred(arg_keys[9], (GROUPS, STATE, GROUP_CH), (2 * GROUP_CH) ** -0.5, 1.0, ((0, 4),), jnp.float32)
    read_re = centred(arg_keys[10], (GROUPS, GROUP_CH, STATE), (2 * STATE) ** -0.5, 0.5, ((0, 4),), jnp.float32)
    read_im = centred(arg_keys[11], (GROUPS, GROUP_CH, STATE), (2 * STATE) ** -0.5, 0.5, ((0, 4),), jnp.float32)
    skip_gain = centred(arg_keys[12], (CH,), 1.0, 4.0, ((0, 4),), jnp.float32)
    glu_weight = centred(arg_keys[13], (CH, CH), CH ** -0.5, 0.1875, ((1, 4),))
    out_proj = centred(arg_keys[14], (CH, D), CH ** -0.5, 0.1875, ((1, 4),))
    ffn_gain = jnp.clip(1.0 + 0.18 * jax.random.normal(arg_keys[15], (D,), jnp.float32), 0.1, 1.9)
    router = centred(arg_keys[16], (D, EXPERTS), D ** -0.5, 0.125, (), jnp.float32)
    gate_weight = centred(arg_keys[17], (EXPERTS, D, FF), (2.5 * D ** -0.5), 0.33007812, ((0, 8), (2, 4)))
    up_weight = centred(arg_keys[18], (EXPERTS, D, FF), (2.5 * D ** -0.5), 0.33007812, ((0, 8), (2, 4)))
    down_weight = heavy_noise(arg_keys[19], (EXPERTS, FF, D), (8 * FF) ** -0.5, 0.046875, ((0, 8), (1, 4)), (1, 2, 4, 2.0))
    route_ids_keys = jax.random.split(jax.random.fold_in(arg_keys[20], 1), SEQS // SEQ_DEV)
    route_ids_turns = jax.random.permutation(jax.random.fold_in(arg_keys[20], 3), SEQS // SEQ_DEV)
    route_ids = jax.vmap(lambda own, number: assign_block(jax.random.fold_in(arg_keys[20], 2), own, number, SEQ_DEV, EXPERTS, TOPK, CAP, 1))(route_ids_keys, route_ids_turns).reshape((SEQS, TOPK))
    return {"residual": residual, "state_re": state_re, "state_im": state_im, "mix_gain": mix_gain, "proj_in": proj_in, "decay_rate": decay_rate, "frequency": frequency, "log_step": log_step, "input_re": input_re, "input_im": input_im, "read_re": read_re, "read_im": read_im, "skip_gain": skip_gain, "glu_weight": glu_weight, "out_proj": out_proj, "ffn_gain": ffn_gain, "router": router, "gate_weight": gate_weight, "up_weight": up_weight, "down_weight": down_weight, "route_ids": route_ids}


EPSILON = 1e-05
LIMIT = 7.0
ALPHA = 1.702

def discretise(decay_rate, frequency, log_step, input_re, input_im):
    real_part = -decay_rate
    imag_part = frequency
    step_size = jnp.exp(log_step)[:, None]
    magnitude = jnp.exp(step_size * real_part)
    abar_re = magnitude * jnp.cos(step_size * imag_part)
    abar_im = magnitude * jnp.sin(step_size * imag_part)
    denom = real_part * real_part + imag_part * imag_part
    minus_one = abar_re - 1.0
    coef_re = (minus_one * real_part + abar_im * imag_part) / denom
    coef_im = (abar_im * real_part - minus_one * imag_part) / denom
    bbar_re = coef_re[..., None] * input_re - coef_im[..., None] * input_im
    bbar_im = coef_re[..., None] * input_im + coef_im[..., None] * input_re
    return (abar_re, abar_im, bbar_re, bbar_im)

def expert_rows(operands):
    tokens, w_gate, w_up, w_down = operands
    gate_pre = jnp.dot(tokens, w_gate, preferred_element_type=jnp.float32)
    up_pre = jnp.dot(tokens, w_up, preferred_element_type=jnp.float32)
    gate_cl = jnp.minimum(gate_pre, LIMIT)
    up_cl = jnp.clip(up_pre, -LIMIT, LIMIT)
    active = ((up_cl + 1.0) * (gate_cl * jax.nn.sigmoid(ALPHA * gate_cl))).astype(jnp.bfloat16)
    rows = active.shape[0]
    block = FF // N_TP
    act_blocks = active.astype(jnp.float32).reshape(rows, N_TP, block)
    down_blocks = w_down.astype(jnp.float32).reshape(N_TP, block, D)
    partial_value = jnp.einsum('rtf,tfd->trd', act_blocks, down_blocks).astype(jnp.bfloat16)
    return lax.optimization_barrier(jnp.sum(partial_value.astype(jnp.float32), axis=0)).astype(jnp.bfloat16)

def reference(residual, state_re, state_im, mix_gain, proj_in, decay_rate, frequency, log_step, input_re, input_im, read_re, read_im, skip_gain, glu_weight, out_proj, ffn_gain, router, gate_weight, up_weight, down_weight, route_ids):
    high = lax.Precision.HIGHEST
    resid_f = residual.astype(jnp.float32)
    scale_one = lax.rsqrt(lax.optimization_barrier(jnp.mean(resid_f * resid_f, axis=1, keepdims=True)) + EPSILON)
    xnorm = (resid_f * scale_one * mix_gain).astype(jnp.bfloat16)
    mix_in = jnp.dot(xnorm, proj_in, preferred_element_type=jnp.float32).astype(jnp.bfloat16)
    mix_f = mix_in.astype(jnp.float32)
    grouped = mix_f.reshape(SEQS, GROUPS, GROUP_CH)
    abar_re, abar_im, bbar_re, bbar_im = discretise(decay_rate, frequency, log_step, input_re, input_im)
    drive_re = jnp.einsum('sgc,gnc->sgn', grouped, bbar_re, precision=high)
    drive_im = jnp.einsum('sgc,gnc->sgn', grouped, bbar_im, precision=high)
    state_re_new = abar_re * state_re - abar_im * state_im + drive_re
    state_im_new = abar_re * state_im + abar_im * state_re + drive_im
    readout = jnp.einsum('sgn,gcn->sgc', state_re_new, read_re, precision=high) - jnp.einsum('sgn,gcn->sgc', state_im_new, read_im, precision=high)
    mixer = jax.nn.gelu(readout.reshape(SEQS, CH) + skip_gain * mix_f, approximate=False)
    glu_gate = jnp.dot(mixer.astype(jnp.bfloat16), glu_weight, preferred_element_type=jnp.float32)
    gated = (mixer * jax.nn.sigmoid(glu_gate)).astype(jnp.bfloat16)
    mixed = jnp.dot(gated, out_proj, preferred_element_type=jnp.float32)
    stream = (resid_f + mixed).astype(jnp.bfloat16)
    stream_f = stream.astype(jnp.float32)
    inverse = lax.rsqrt(lax.optimization_barrier(jnp.mean(stream_f * stream_f, axis=1, keepdims=True)) + EPSILON)
    normed = (stream_f * inverse * ffn_gain).astype(jnp.bfloat16)
    logits = jnp.dot(stream_f * ffn_gain, router, precision=high) * inverse
    picked = jnp.take_along_axis(logits, route_ids, axis=1)
    expon = jnp.exp(picked)
    weights = expon / lax.optimization_barrier(jnp.sum(expon, axis=1, keepdims=True))
    flat_route = route_ids.reshape(N_EP, SEQ_DEV * TOPK).astype(jnp.int32)
    one_hot = (flat_route[..., None] == jnp.arange(EXPERTS, dtype=jnp.int32)).astype(jnp.int32)
    before = jnp.cumsum(one_hot, axis=1) - one_hot
    slot_ids = lax.optimization_barrier(jnp.sum(before * one_hot, axis=2)).astype(jnp.int32)
    source = jnp.broadcast_to(jnp.arange(N_EP, dtype=jnp.int32)[:, None], flat_route.shape)
    tokens = jnp.broadcast_to(normed.reshape(N_EP, SEQ_DEV, 1, D), (N_EP, SEQ_DEV, TOPK, D))
    tokens = tokens.reshape(N_EP, SEQ_DEV * TOPK, D)
    buffer = jnp.zeros((EXPERTS, N_EP, CAP, D), jnp.bfloat16)
    buffer = buffer.at[flat_route, source, slot_ids].set(tokens)
    results = lax.map(expert_rows, (buffer.reshape(EXPERTS, N_EP * CAP, D), gate_weight, up_weight, down_weight))
    results = results.reshape(EXPERTS, N_EP, CAP, D)
    fetched = results[flat_route, source, slot_ids].astype(jnp.float32).reshape(SEQS, TOPK, D)
    experts_sum = lax.optimization_barrier(jnp.sum(weights[..., None] * fetched, axis=1))
    layer_out = (stream_f + experts_sum).astype(jnp.bfloat16)
    return (layer_out, state_re_new, state_im_new)
```

```python
import functools

import jax
import jax.numpy as jnp
from jax import lax
from jax.experimental import pallas as pl
from jax.experimental.pallas import tpu as pltpu
from jax.sharding import PartitionSpec as P

EPSILON = 1e-05
LIMIT = 7.0
ALPHA = 1.702


def discretise(decay_rate, frequency, log_step, input_re, input_im):
    real_part = -decay_rate
    step_size = jnp.exp(log_step)[:, None]
    magnitude = jnp.exp(step_size * real_part)
    abar_re = magnitude * jnp.cos(step_size * frequency)
    abar_im = magnitude * jnp.sin(step_size * frequency)
    denom = real_part * real_part + frequency * frequency
    minus_one = abar_re - 1.0
    coef_re = (minus_one * real_part + abar_im * frequency) / denom
    coef_im = (abar_im * real_part - minus_one * frequency) / denom
    bbar_re = coef_re[..., None] * input_re - coef_im[..., None] * input_im
    bbar_im = coef_re[..., None] * input_im + coef_im[..., None] * input_re
    return (abar_re, abar_im, bbar_re, bbar_im)


def per_device(
    residual,
    state_re,
    state_im,
    mix_gain,
    proj_in,
    decay_rate,
    frequency,
    log_step,
    input_re,
    input_im,
    read_re,
    read_im,
    skip_gain,
    glu_weight,
    out_proj,
    ffn_gain,
    router,
    gate_weight,
    up_weight,
    down_weight,
    route_ids,
):
    high = lax.Precision.HIGHEST
    seq_rows = residual.shape[0]
    col_count = residual.shape[1]
    width = mix_gain.shape[0]
    ep_size = lax.axis_size("ep")
    own_resid = residual.astype(jnp.float32)
    full_resid = lax.all_gather(residual, "tp", axis=1, tiled=True).astype(jnp.float32)
    scale_one = lax.rsqrt(jnp.mean(full_resid * full_resid, axis=1, keepdims=True) + EPSILON)
    xnorm = (full_resid * scale_one * mix_gain).astype(jnp.bfloat16)
    mix_in = jnp.dot(xnorm, proj_in, preferred_element_type=jnp.float32).astype(jnp.bfloat16)
    mix_f = mix_in.astype(jnp.float32)
    group_count = decay_rate.shape[0]
    group_width = input_re.shape[2]
    grouped = mix_f.reshape(seq_rows, group_count, group_width)
    abar_re, abar_im, bbar_re, bbar_im = discretise(
        decay_rate, frequency, log_step, input_re, input_im
    )
    drive_re = jnp.einsum("sgc,gnc->sgn", grouped, bbar_re, precision=high)
    drive_im = jnp.einsum("sgc,gnc->sgn", grouped, bbar_im, precision=high)
    state_re_new = abar_re * state_re - abar_im * state_im + drive_re
    state_im_new = abar_re * state_im + abar_im * state_re + drive_im
    readout = jnp.einsum("sgn,gcn->sgc", state_re_new, read_re, precision=high) - jnp.einsum(
        "sgn,gcn->sgc", state_im_new, read_im, precision=high
    )
    mixer = jax.nn.gelu(
        readout.reshape(seq_rows, group_count * group_width) + skip_gain * mix_f, approximate=False
    )
    all_mixer = lax.all_gather(mixer.astype(jnp.bfloat16), "tp", axis=1, tiled=True)
    glu_gate = jnp.dot(all_mixer, glu_weight, preferred_element_type=jnp.float32)
    gated = (mixer * jax.nn.sigmoid(glu_gate)).astype(jnp.bfloat16)
    all_gated = lax.all_gather(gated, "tp", axis=1, tiled=True)
    mixed = jnp.dot(all_gated, out_proj, preferred_element_type=jnp.float32)
    stream = (own_resid + mixed).astype(jnp.bfloat16)
    stream_f = stream.astype(jnp.float32)
    all_stream = lax.all_gather(stream, "tp", axis=1, tiled=True).astype(jnp.float32)
    inverse = lax.rsqrt(jnp.mean(all_stream * all_stream, axis=1, keepdims=True) + EPSILON)
    logits = jnp.dot(all_stream * ffn_gain, router, precision=high) * inverse
    payload = (all_stream * inverse * ffn_gain).astype(jnp.bfloat16)
    expert_count = router.shape[1]
    top_count = route_ids.shape[1]
    capacity = seq_rows * top_count // expert_count + 1
    expert_iota = jnp.arange(expert_count, dtype=jnp.int32)
    choose = (route_ids[:, :, None] == expert_iota).astype(jnp.float32)
    picked = jnp.sum(choose * logits[:, None, :], axis=2)
    expon = jnp.exp(picked)
    weights = expon / jnp.sum(expon, axis=1, keepdims=True)
    flat_route = route_ids.reshape(seq_rows * top_count)
    one_hot = (flat_route[:, None] == expert_iota).astype(jnp.int32)
    before = jnp.cumsum(one_hot, axis=0) - one_hot
    slot_ids = jnp.sum(before * one_hot, axis=1)
    target = flat_route * capacity + slot_ids
    slot_iota = jnp.arange(expert_count * capacity, dtype=jnp.int32)
    placing = jnp.any(slot_iota[:, None, None] == target.reshape(seq_rows, top_count)[None], axis=2)
    buffer = jnp.dot(placing.astype(jnp.bfloat16), payload, preferred_element_type=jnp.float32)
    buffer = buffer.astype(jnp.bfloat16).reshape(expert_count, capacity, payload.shape[1])
    local_experts = gate_weight.shape[0]
    received = lax.all_to_all(buffer, "ep", split_axis=0, concat_axis=0, tiled=True)
    items = received.shape[1]
    tokens = received.reshape(ep_size, local_experts, items, width)
    tokens = tokens.transpose(1, 0, 2, 3).reshape(local_experts, ep_size * items, width)
    gate_pre = jnp.einsum("esd,edf->esf", tokens, gate_weight, preferred_element_type=jnp.float32)
    up_pre = jnp.einsum("esd,edf->esf", tokens, up_weight, preferred_element_type=jnp.float32)
    gate_cl = jnp.minimum(gate_pre, LIMIT)
    up_cl = jnp.clip(up_pre, -LIMIT, LIMIT)
    active = ((up_cl + 1.0) * (gate_cl * jax.nn.sigmoid(ALPHA * gate_cl))).astype(jnp.bfloat16)
    partial_value = jnp.einsum(
        "esf,efd->esd", active, down_weight, preferred_element_type=jnp.float32
    ).astype(jnp.bfloat16)
    summed = lax.psum_scatter(
        partial_value.astype(jnp.float32).astype(jnp.bfloat16),
        "tp",
        scatter_dimension=2,
        tiled=True,
    )
    outgoing = summed.reshape(local_experts, ep_size, items, col_count)
    outgoing = outgoing.transpose(1, 0, 2, 3).reshape(ep_size * local_experts, items, col_count)
    returned = lax.all_to_all(outgoing, "ep", split_axis=0, concat_axis=0, tiled=True)
    flat_back = returned.reshape(expert_count * capacity, col_count)
    fetched = (
        jnp.take(flat_back, target, axis=0)
        .astype(jnp.float32)
        .reshape(seq_rows, top_count, col_count)
    )
    experts_sum = jnp.sum(weights[..., None] * fetched, axis=1)
    layer_out = (stream_f + experts_sum).astype(jnp.bfloat16)
    return (layer_out, state_re_new, state_im_new)


def erf(x):
    x = jnp.clip(x, -3.832506856900711, 3.832506856900711)
    y = x * x
    top = 0.00022905065861350646
    for coefficient in (
        0.0034082910107109506,
        0.050955695062380861,
        0.18520832239976145,
        1.128379143519084,
    ):
        top = top * y + coefficient
    bottom = -1.1791602954361697e-7
    for coefficient in (
        0.000023547966471313185,
        0.0010179625278914885,
        0.014070470171167667,
        0.11098505178285362,
        0.49746925110067538,
        1.0,
    ):
        bottom = bottom * y + coefficient
    return x * top / bottom


def layer_kernel(
    sizes,
    resid_ref,
    gain1_ref,
    decay_ref,
    freq_ref,
    step_ref,
    in_re_ref,
    in_im_ref,
    read_re_ref,
    read_im_ref,
    skip_ref,
    gain2_ref,
    router_ref,
    route_ref,
    sre_hbm,
    sim_hbm,
    proj_hbm,
    glu_hbm,
    outp_hbm,
    gate_hbm,
    up_hbm,
    down_hbm,
    out_ref,
    sre_out,
    sim_out,
    sre,
    sim,
    proj,
    glu,
    outp,
    wg,
    wu,
    wd,
    res_all,
    mix_all,
    gated_all,
    logit_all,
    place_all,
    weight_all,
    pick,
    spill,
    tok,
    acc_g,
    acc_u,
    act,
    mine,
    sib_out,
    sib_in,
    summed,
    from_side,
    fwd_in,
    fwd_out,
    home_out,
    home_in,
    load_sem,
    store_sem,
    send_sem,
    recv_sem,
):
    ep, tp, cap, rows = sizes
    f32, bf16 = jnp.float32, jnp.bfloat16
    me, t = lax.axis_index("ep"), lax.axis_index("tp")
    seqs, cols = resid_ref.shape
    width = cols * tp
    groups, states = decay_ref.shape
    chans = skip_ref.shape[1]
    group_width = chans // groups
    chips = ep // 2
    pair = 2 * seqs
    half = seqs // 2
    last = (((1,), (1,)), ((), ()))

    def dot(a, b):
        return jnp.dot(a, b, preferred_element_type=f32)

    loads = [
        pltpu.make_async_copy(a, b, load_sem.at[n])
        for n, (a, b) in enumerate(
            [
                (proj_hbm, proj),
                (sre_hbm, sre),
                (sim_hbm, sim),
                (glu_hbm, glu),
                (outp_hbm, outp),
                (gate_hbm, wg),
                (up_hbm, wu),
            ]
            + [(down_hbm.at[:, j * cols : (j + 1) * cols], wd.at[j]) for j in range(tp)]
        )
    ]
    for load in loads:
        load.start()

    barrier = pltpu.get_barrier_semaphore()
    for k in range(1, tp):
        pl.semaphore_signal(barrier, inc=1, device_id=(me, (t + k) % tp), device_id_type=pl.DeviceIdType.MESH)
    for k in range(1, ep):
        pl.semaphore_signal(barrier, inc=1, device_id=((me + k) % ep, t), device_id_type=pl.DeviceIdType.MESH)
    pl.semaphore_wait(barrier, tp + ep - 2)

    copies = []

    def remote(source, target, peer):
        n = len(copies)
        copy = pltpu.make_async_remote_copy(
            src_ref=source,
            dst_ref=target,
            send_sem=send_sem.at[n],
            recv_sem=recv_sem.at[n],
            device_id=peer,
            device_id_type=pl.DeviceIdType.MESH,
        )
        copy.start()
        copies.append(copy)
        return copy

    def flip(value, k):
        for bit in (1, 2, 4, 8, 16):
            if k & bit:
                value = value + bit - 2 * bit * ((value // bit) % 2)
        return value

    beside, across = flip(t, 1), flip(t, 2)
    opposite = flip(beside, 2)
    sibling = flip(me, 1)
    side_b, side_a, twin = (me, beside), (me, across), (sibling, t)

    def gather(source, target):
        return [remote(source, target, (me, flip(t, k))) for k in (3, 1, 2)]

    gather0 = gather(resid_ref, res_all.at[t])
    res_all[t] = resid_ref[...]

    square = (groups, groups)
    diagonal = lax.broadcasted_iota(jnp.int32, square, 0) == lax.broadcasted_iota(jnp.int32, square, 1)
    log_step = jnp.sum(
        jnp.where(diagonal, jnp.broadcast_to(step_ref[...], square), 0.0), axis=1, keepdims=True
    )
    step_size = jnp.exp(log_step)
    real_part, imag_part = -decay_ref[...], freq_ref[...]
    magnitude = jnp.exp(step_size * real_part)
    abar_re = magnitude * jnp.cos(step_size * imag_part)
    abar_im = magnitude * jnp.sin(step_size * imag_part)
    denom = real_part * real_part + imag_part * imag_part
    minus_one = abar_re - 1.0
    coef_re = ((minus_one * real_part + abar_im * imag_part) / denom)[:, None, :]
    coef_im = ((abar_im * real_part - minus_one * imag_part) / denom)[:, None, :]
    in_re, in_im = in_re_ref[...], in_im_ref[...]
    bb_re = (coef_re * in_re - coef_im * in_im).astype(bf16).reshape(chans, states)
    bb_im = (coef_re * in_im + coef_im * in_re).astype(bf16).reshape(chans, states)
    abar_re, abar_im = abar_re[None], abar_im[None]

    route = route_ref[...]
    iota_e = lax.broadcasted_iota(jnp.int32, (ep, seqs), 0)
    routed_t = jnp.zeros((ep, seqs), f32)
    for j in range(route.shape[0]):
        routed_t = routed_t + jnp.where(route[j : j + 1, :] == iota_e, 1.0, 0.0)
    row_i = lax.broadcasted_iota(jnp.int32, (seqs, seqs), 0)
    col_i = lax.broadcasted_iota(jnp.int32, (seqs, seqs), 1)
    earlier_t = dot(routed_t.astype(bf16), jnp.where(row_i < col_i, 1.0, 0.0).astype(bf16))
    place_all[0, 0] = jnp.zeros(place_all.shape[2:], f32)
    place_all[0, 0, :, 0:seqs] = jnp.where(routed_t > 0.5, earlier_t, -5000.0)
    peers = [(n, twin_bit) for n in range(chips) for twin_bit in range(2)][1:]
    place_copies = {
        (n, b): remote(place_all.at[0, 0], place_all.at[n, b], (flip(me, 2 * n + b), t)) for n, b in peers
    }

    loads[0].wait()
    for copy in gather0:
        copy.wait_recv()
    total = jnp.zeros((seqs, 1), f32)
    for j in range(tp):
        part = res_all[j].astype(f32)
        total = total + jnp.sum(part * part, axis=1, keepdims=True)
    scale = lax.rsqrt(total / width + EPSILON)
    mix = jnp.zeros((seqs, chans), f32)
    for j in range(tp):
        xnorm = (res_all[j].astype(f32) * scale * gain1_ref[j]).astype(bf16)
        mix = mix + dot(xnorm, proj[j * cols : (j + 1) * cols, :])
    mix_f = mix.astype(bf16).astype(f32)
    lane_c = lax.broadcasted_iota(jnp.int32, (seqs, groups, chans), 2)
    group_c = lax.broadcasted_iota(jnp.int32, (seqs, groups, chans), 1)
    first = group_c * group_width
    own = (lane_c >= first) & (lane_c < first + group_width)
    spread = jnp.where(own, jnp.broadcast_to(mix_f[:, None, :], own.shape), 0.0)
    spread = spread.astype(bf16).reshape(seqs * groups, chans)
    drive_re = dot(spread, bb_re).reshape(seqs, groups, states)
    drive_im = dot(spread, bb_im).reshape(seqs, groups, states)
    loads[1].wait()
    loads[2].wait()
    old_re, old_im = sre[...], sim[...]
    new_re = abar_re * old_re - abar_im * old_im + drive_re
    new_im = abar_re * old_im + abar_im * old_re + drive_im
    sre[...] = new_re
    sim[...] = new_im
    stores = [
        pltpu.make_async_copy(sre, sre_out, store_sem.at[0]),
        pltpu.make_async_copy(sim, sim_out, store_sem.at[1]),
    ]
    for store in stores:
        store.start()
    flat = (seqs * groups, states)
    readout = lax.dot_general(
        new_re.reshape(flat).astype(bf16), read_re_ref[...].astype(bf16), last, preferred_element_type=f32
    ) - lax.dot_general(
        new_im.reshape(flat).astype(bf16), read_im_ref[...].astype(bf16), last, preferred_element_type=f32
    )
    readout = jnp.sum(jnp.where(own, readout.reshape(seqs, groups, chans), 0.0), axis=1)
    pre = readout + skip_ref[...] * mix_f
    mixer = 0.5 * pre * (1.0 + erf(pre * 0.7071067811865476))
    mix_all[t] = mixer.astype(bf16)
    gather1 = gather(mix_all.at[t], mix_all.at[t])

    for copy in place_copies.values():
        copy.wait_recv()
    iota_r = lax.broadcasted_iota(jnp.int32, (rows, seqs), 0).astype(f32)
    iota_l = lax.broadcasted_iota(jnp.int32, (seqs, rows), 1).astype(f32)

    def slot_row(n, b):
        return place_all[n, b, pl.ds(me, 1), 0:seqs] + float((n % 2 * 2 + b) * cap)

    for n in range(chips):
        for b in range(2):
            slots = slot_row(n, b)
            span = slice((n % 2 * 2 + b) * seqs, (n % 2 * 2 + b + 1) * seqs)
            pick[n // 2, :, span] = jnp.where(iota_r == slots, 1.0, 0.0).astype(bf16)
            down = jnp.sum(jnp.where(row_i == col_i, slots, 0.0), axis=1, keepdims=True)
            spill[n, b * seqs : (b + 1) * seqs, :] = jnp.where(iota_l == down, 1.0, 0.0).astype(bf16)

    loads[3].wait()
    for copy in gather1:
        copy.wait_recv()
    glu_gate = jnp.zeros((seqs, chans), f32)
    for j in range(tp):
        glu_gate = glu_gate + dot(mix_all[j], glu[j * chans : (j + 1) * chans, :])
    gated_all[t] = (mixer * jax.nn.sigmoid(glu_gate)).astype(bf16)
    gather2 = gather(gated_all.at[t], gated_all.at[t])
    loads[4].wait()
    for copy in gather2:
        copy.wait_recv()
    mixed = resid_ref[...].astype(f32)
    for j in range(tp):
        mixed = mixed + dot(gated_all[j], outp[j * chans : (j + 1) * chans, :])
    stream = mixed.astype(bf16)
    stream_f = stream.astype(f32)

    def place_of(n, b):
        return pl.ds((n % 2) * pair + b * seqs, seqs)

    tok[0, t, 0:seqs, :] = stream
    here = {}
    twin_in = {}

    def slab(n, j, b=0, cut=None):
        begin, size = (n % 2) * pair + b * seqs, seqs
        if cut is not None:
            begin, size = begin + cut * half, half
        return tok.at[n // 2, j, pl.ds(begin, size)]

    def to_twin(n, key, j, cut=None):
        twin_in[n, key] = remote(slab(n, j, 0, cut), slab(n, j, 1, cut), twin)

    def spread_chips():
        for n in range(1, chips):
            here[n, "z"] = remote(slab(0, t), slab(n, t), (flip(me, 2 * n), t))

    def enter(n):
        if n:
            here[n, "z"].wait_recv()
        here[n, "b"] = remote(slab(n, t), slab(n, t), side_b)
        here[n, "a"] = remote(slab(n, t), slab(n, t), side_a)
        to_twin(n, "t", t)

    def relay(n):
        here[n, "b"].wait_recv()
        here[n, "ob"] = remote(slab(n, beside, 0, 0), slab(n, beside, 0, 0), side_a)
        to_twin(n, "b", beside)
        here[n, "a"].wait_recv()
        here[n, "oa"] = remote(slab(n, across, 0, 1), slab(n, across, 0, 1), side_b)
        to_twin(n, "a", across)

    def corner(n):
        here[n, "ob"].wait_recv()
        to_twin(n, "o0", opposite, 0)
        here[n, "oa"].wait_recv()
        to_twin(n, "o1", opposite, 1)

    def logits():
        logit_all[t] = jnp.zeros(logit_all.shape[1:], f32)
        logit_all[t, 0:ep, 0:seqs] = lax.dot_general(
            router_ref[:, pl.ds(pl.multiple_of(t * cols, cols), cols)],
            stream_f * gain2_ref[t],
            last,
            precision=lax.Precision.HIGHEST,
            preferred_element_type=f32,
        )
        energy = jnp.sum(stream_f * stream_f, axis=1, keepdims=True)
        logit_all[t, ep : ep + 1, 0:seqs] = jnp.sum(
            jnp.where(row_i == col_i, energy, 0.0), axis=0, keepdims=True
        )
        here["logits"] = gather(logit_all.at[t], logit_all.at[t])

    def weights():
        for copy in here["logits"]:
            copy.wait_recv()
        whole = logit_all[0]
        for j in range(1, tp):
            whole = whole + logit_all[j]
        whole = whole[:, 0:seqs]
        inverse = lax.rsqrt(whole[ep : ep + 1] / width + EPSILON)
        chosen = routed_t > 0.5
        expon = jnp.where(chosen, jnp.exp(jnp.where(chosen, whole[0:ep] * inverse, 0.0)), 0.0)
        weight_all[0, 0] = jnp.zeros(weight_all.shape[2:], f32)
        weight_all[0, 0, 0:ep, 0:seqs] = expon / jnp.sum(expon, axis=0, keepdims=True)
        weight_all[0, 0, ep : ep + 1, 0:seqs] = inverse
        for n, b in peers:
            here["w", n, b] = remote(weight_all.at[0, 0], weight_all.at[n, b], (flip(me, 2 * n + b), t))

    def expert_in(h, block):
        j = {"t": t, "b": beside, "a": across, "o": opposite}[block]
        if (h, block) == (0, "t"):
            loads[5].wait()
            loads[6].wait()
        for n in (2 * h, 2 * h + 1):
            for key in ("o0", "o1") if block == "o" else (block,):
                twin_in[n, key].wait_recv()
        part = dot(pick[h], tok[h, j])
        scaled = (part * gain2_ref[j]).astype(bf16)
        span = pl.ds(pl.multiple_of(j * cols, cols), cols)
        if block == "t":
            acc_g[...] = dot(scaled, wg[span, :])
            acc_u[...] = dot(scaled, wu[span, :])
        else:
            acc_g[...] += dot(scaled, wg[span, :])
            acc_u[...] += dot(scaled, wu[span, :])

    def activate(h):
        norm = jnp.zeros((rows, 1), f32)
        share = jnp.zeros((rows, 1), f32)
        for n in (2 * h, 2 * h + 1):
            for b in range(2):
                if (n, b) != (0, 0):
                    here["w", n, b].wait_recv()
                match = iota_r == slot_row(n, b)
                inverse = weight_all[n, b, ep : ep + 1, 0:seqs]
                weight = weight_all[n, b, pl.ds(me, 1), 0:seqs]
                norm = norm + jnp.sum(jnp.where(match, inverse, 0.0), axis=1, keepdims=True)
                share = share + jnp.sum(jnp.where(match, weight, 0.0), axis=1, keepdims=True)
        gate_cl = jnp.minimum(acc_g[...] * norm, LIMIT)
        up_cl = jnp.clip(acc_u[...] * norm, -LIMIT, LIMIT)
        act[h] = (((up_cl + 1.0) * share) * (gate_cl * jax.nn.sigmoid(ALPHA * gate_cl))).astype(bf16)

    def expert_out(n):
        if n == firsts[0]:
            for load in loads[7:]:
                load.wait()
        spread_act = dot(spill[n], act[n // 2]).astype(bf16)
        for key, j in (("o", opposite), ("b", beside), ("a", across), ("t", t)):
            value = dot(spread_act, wd[j])
            sib_out[n, j] = value[seqs:].astype(bf16)
            here[n, "s" + key] = remote(sib_out.at[n, j], sib_in.at[n, j], twin)
            mine[n, j] = value[:seqs]

    def reduce_chip(n):
        here[n, "so"].wait_recv()
        summed[n, opposite] = (mine[n, opposite] + sib_in[n, opposite].astype(f32)).astype(bf16)
        top, bottom = pl.ds(0, half), pl.ds(half, half)
        here[n, "fb"] = remote(summed.at[n, opposite, top], fwd_in.at[n, 0], side_b)
        here[n, "fa"] = remote(summed.at[n, opposite, bottom], fwd_in.at[n, 1], side_a)
        here[n, "sb"].wait_recv()
        both = mine[n, beside] + sib_in[n, beside].astype(f32)
        mine[n, beside] = both
        summed[n, beside, 0:half] = both[0:half].astype(bf16)
        here[n, "db"] = remote(summed.at[n, beside, top], from_side.at[n, 0, top], side_b)
        here[n, "sa"].wait_recv()
        both = mine[n, across] + sib_in[n, across].astype(f32)
        mine[n, across] = both
        summed[n, across, half:] = both[half:].astype(bf16)
        here[n, "da"] = remote(summed.at[n, across, bottom], from_side.at[n, 1, bottom], side_a)

    def reduce_relay(n):
        top, bottom = pl.ds(0, half), pl.ds(half, half)
        here[n, "fb"].wait_recv()
        fwd_out[n, 0] = (mine[n, across, 0:half] + fwd_in[n, 0].astype(f32)).astype(bf16)
        here[n, "ga"] = remote(fwd_out.at[n, 0], from_side.at[n, 1, top], side_a)
        here[n, "fa"].wait_recv()
        fwd_out[n, 1] = (mine[n, beside, half:] + fwd_in[n, 1].astype(f32)).astype(bf16)
        here[n, "gb"] = remote(fwd_out.at[n, 1], from_side.at[n, 0, bottom], side_b)

    def go_home(n):
        here[n, "st"].wait_recv()
        value = mine[n, t] + sib_in[n, t].astype(f32)
        for key in ("db", "da", "ga", "gb"):
            here[n, key].wait_recv()
        value = value + from_side[n, 0].astype(f32) + from_side[n, 1].astype(f32)
        if n:
            home_out[n] = value.astype(bf16)
            here[n, "h"] = remote(home_out.at[n], home_in.at[n], (flip(me, 2 * n), t))
        else:
            mine[n, t] = value

    def finish():
        result = stream_f + mine[0, t]
        for n in range(1, chips):
            here[n, "h"].wait_recv()
            result = result + home_in[n].astype(f32)
        out_ref[...] = result.astype(bf16)

    firsts = (1,)
    plan = [
        (spread_chips,), (enter, 0), (logits,),
        (enter, 1), (relay, 0), (weights,), (corner, 0), (enter, 2), (relay, 1),
        (expert_in, 0, "t"), (enter, 3), (corner, 1), (expert_in, 0, "b"), (relay, 2), (expert_in, 0, "a"),
        (expert_in, 0, "o"), (corner, 2), (relay, 3), (activate, 0), (expert_out, 1), (corner, 3), (expert_out, 0),
        (reduce_chip, 1), (expert_in, 1, "t"), (reduce_chip, 0), (expert_in, 1, "b"), (reduce_relay, 1), (expert_in, 1, "a"),
        (reduce_relay, 0), (expert_in, 1, "o"), (activate, 1), (expert_out, 3), (go_home, 1), (expert_out, 2),
        (go_home, 0), (reduce_chip, 3), (reduce_chip, 2), (reduce_relay, 3), (reduce_relay, 2), (go_home, 3), (go_home, 2),
        (finish,),
    ]
    for step in plan:
        step[0](*step[1:])
    for copy in copies:
        copy.wait_send()
    for store in stores:
        store.wait()


def finish_kernel(a_in, b_in, c_in, a_out, b_out, c_out, a, b, c, sems):
    reads = [
        pltpu.make_async_copy(source, held, sems.at[n])
        for n, (source, held) in enumerate(((a_in, a), (b_in, b), (c_in, c)))
    ]
    writes = [
        pltpu.make_async_copy(held, target, sems.at[3 + n])
        for n, (held, target) in enumerate(((a, a_out), (b, b_out), (c, c_out)))
    ]
    for read in reads:
        read.start()
    for read, write in zip(reads, writes):
        read.wait()
        write.start()
    for write in writes:
        write.wait()


def dispatch(*args):
    (
        residual, state_re, state_im, mix_gain, proj_in, decay_rate, frequency, log_step,
        input_re, input_im, read_re, read_im, skip_gain, glu_weight, out_proj, ffn_gain,
        router, gate_weight, up_weight, down_weight, route_ids,
    ) = args
    ep, tp = lax.axis_size("ep"), lax.axis_size("tp")
    seqs, cols = residual.shape
    groups, states = decay_rate.shape
    chans = skip_gain.shape[0]
    rough = groups % 16 or chans % 128 or cols % 128 or seqs % 32 or seqs > 128
    if gate_weight.shape[0] != 1 or tp != 4 or ep != 8 or rough:
        return per_device(*args)
    top = route_ids.shape[1]
    cap = seqs * top // router.shape[1] + 1
    rows = -(-4 * cap // 16) * 16
    hidden = gate_weight.shape[2]
    chips = ep // 2
    halves = chips // 2
    bf16, f32 = jnp.bfloat16, jnp.float32
    vmem, anywhere = pl.BlockSpec(memory_space=pltpu.VMEM), pl.BlockSpec(memory_space=pl.ANY)
    state_shape = (seqs, groups, states)
    blocks = (chips, tp, seqs, cols)
    out = pl.pallas_call(
        functools.partial(layer_kernel, (ep, tp, cap, rows)),
        out_shape=(
            jax.ShapeDtypeStruct((seqs, cols), bf16),
            jax.ShapeDtypeStruct(state_shape, f32),
            jax.ShapeDtypeStruct(state_shape, f32),
        ),
        in_specs=[vmem] * 13 + [anywhere] * 8,
        out_specs=(vmem, anywhere, anywhere),
        scratch_shapes=[
            pltpu.VMEM(state_shape, f32),
            pltpu.VMEM(state_shape, f32),
            pltpu.VMEM(proj_in.shape, bf16),
            pltpu.VMEM(glu_weight.shape, bf16),
            pltpu.VMEM(out_proj.shape, bf16),
            pltpu.VMEM(gate_weight.shape[1:], bf16),
            pltpu.VMEM(up_weight.shape[1:], bf16),
            pltpu.VMEM((tp, hidden, cols), bf16),
            pltpu.VMEM((tp, seqs, cols), bf16),
            pltpu.VMEM((tp, seqs, chans), bf16),
            pltpu.VMEM((tp, seqs, chans), bf16),
            pltpu.VMEM((tp, 2 * ep, 128), f32),
            pltpu.VMEM((chips, 2, ep, 128), f32),
            pltpu.VMEM((chips, 2, 2 * ep, 128), f32),
            pltpu.VMEM((halves, rows, 4 * seqs), bf16),
            pltpu.VMEM((chips, 2 * seqs, rows), bf16),
            pltpu.VMEM((halves, tp, 4 * seqs, cols), bf16),
            pltpu.VMEM((rows, hidden), f32),
            pltpu.VMEM((rows, hidden), f32),
            pltpu.VMEM((halves, rows, hidden), bf16),
            pltpu.VMEM(blocks, f32),
            pltpu.VMEM(blocks, bf16),
            pltpu.VMEM(blocks, bf16),
            pltpu.VMEM(blocks, bf16),
            pltpu.VMEM((chips, 2, seqs, cols), bf16),
            pltpu.VMEM((chips, 2, seqs // 2, cols), bf16),
            pltpu.VMEM((chips, 2, seqs // 2, cols), bf16),
            pltpu.VMEM((chips, seqs, cols), bf16),
            pltpu.VMEM((chips, seqs, cols), bf16),
            pltpu.SemaphoreType.DMA((7 + tp,)),
            pltpu.SemaphoreType.DMA((2,)),
            pltpu.SemaphoreType.DMA((128,)),
            pltpu.SemaphoreType.DMA((128,)),
        ],
        compiler_params=pltpu.CompilerParams(
            collective_id=0, has_side_effects=True, vmem_limit_bytes=60 * 1024 * 1024
        ),
        name="layer",
    )(
        residual,
        mix_gain.reshape(tp, 1, cols),
        decay_rate,
        frequency,
        log_step.reshape(1, groups),
        input_re.transpose(0, 2, 1),
        input_im.transpose(0, 2, 1),
        read_re.reshape(chans, states),
        read_im.reshape(chans, states),
        skip_gain.reshape(1, chans),
        ffn_gain.reshape(tp, 1, cols),
        router.T,
        route_ids.T,
        state_re,
        state_im,
        proj_in,
        glu_weight,
        out_proj,
        gate_weight.reshape(gate_weight.shape[1:]),
        up_weight.reshape(up_weight.shape[1:]),
        down_weight.reshape(down_weight.shape[1:]),
    )
    return pl.pallas_call(
        finish_kernel,
        out_shape=tuple(jax.ShapeDtypeStruct(part.shape, part.dtype) for part in out),
        in_specs=[anywhere] * 3,
        out_specs=(anywhere,) * 3,
        scratch_shapes=[pltpu.VMEM(part.shape, part.dtype) for part in out]
        + [pltpu.SemaphoreType.DMA((6,))],
        name="finish",
    )(*out)


def solution(mesh):
    in_specs = (
        P("ep", "tp"),
        P("ep", "tp", None),
        P("ep", "tp", None),
        P(),
        P(None, "tp"),
        P("tp", None),
        P("tp", None),
        P("tp"),
        P("tp", None, None),
        P("tp", None, None),
        P("tp", None, None),
        P("tp", None, None),
        P("tp"),
        P(None, "tp"),
        P(None, "tp"),
        P(),
        P(),
        P("ep", None, "tp"),
        P("ep", None, "tp"),
        P("ep", "tp", None),
        P("ep", None),
    )
    out_specs = (P("ep", "tp"), P("ep", "tp", None), P("ep", "tp", None))
    return jax.shard_map(
        dispatch, mesh=mesh, in_specs=in_specs, out_specs=out_specs, check_vma=False
    )
```

```python
import functools

import jax
import jax.numpy as jnp
from jax import lax
from jax.experimental import pallas as pl
from jax.experimental.pallas import tpu as pltpu
from jax.sharding import PartitionSpec as P

EPSILON = 1e-05
LIMIT = 7.0
ALPHA = 1.702


def discretise(decay_rate, frequency, log_step, input_re, input_im):
    real_part = -decay_rate
    step_size = jnp.exp(log_step)[:, None]
    magnitude = jnp.exp(step_size * real_part)
    abar_re = magnitude * jnp.cos(step_size * frequency)
    abar_im = magnitude * jnp.sin(step_size * frequency)
    denom = real_part * real_part + frequency * frequency
    minus_one = abar_re - 1.0
    coef_re = (minus_one * real_part + abar_im * frequency) / denom
    coef_im = (abar_im * real_part - minus_one * frequency) / denom
    bbar_re = coef_re[..., None] * input_re - coef_im[..., None] * input_im
    bbar_im = coef_re[..., None] * input_im + coef_im[..., None] * input_re
    return (abar_re, abar_im, bbar_re, bbar_im)


def per_device(
    residual,
    state_re,
    state_im,
    mix_gain,
    proj_in,
    decay_rate,
    frequency,
    log_step,
    input_re,
    input_im,
    read_re,
    read_im,
    skip_gain,
    glu_weight,
    out_proj,
    ffn_gain,
    router,
    gate_weight,
    up_weight,
    down_weight,
    route_ids,
):
    high = lax.Precision.HIGHEST
    seq_rows = residual.shape[0]
    col_count = residual.shape[1]
    width = mix_gain.shape[0]
    ep_size = lax.axis_size("ep")
    own_resid = residual.astype(jnp.float32)
    full_resid = lax.all_gather(residual, "tp", axis=1, tiled=True).astype(jnp.float32)
    scale_one = lax.rsqrt(jnp.mean(full_resid * full_resid, axis=1, keepdims=True) + EPSILON)
    xnorm = (full_resid * scale_one * mix_gain).astype(jnp.bfloat16)
    mix_in = jnp.dot(xnorm, proj_in, preferred_element_type=jnp.float32).astype(jnp.bfloat16)
    mix_f = mix_in.astype(jnp.float32)
    group_count = decay_rate.shape[0]
    group_width = input_re.shape[2]
    grouped = mix_f.reshape(seq_rows, group_count, group_width)
    abar_re, abar_im, bbar_re, bbar_im = discretise(
        decay_rate, frequency, log_step, input_re, input_im
    )
    drive_re = jnp.einsum("sgc,gnc->sgn", grouped, bbar_re, precision=high)
    drive_im = jnp.einsum("sgc,gnc->sgn", grouped, bbar_im, precision=high)
    state_re_new = abar_re * state_re - abar_im * state_im + drive_re
    state_im_new = abar_re * state_im + abar_im * state_re + drive_im
    readout = jnp.einsum("sgn,gcn->sgc", state_re_new, read_re, precision=high) - jnp.einsum(
        "sgn,gcn->sgc", state_im_new, read_im, precision=high
    )
    mixer = jax.nn.gelu(
        readout.reshape(seq_rows, group_count * group_width) + skip_gain * mix_f, approximate=False
    )
    all_mixer = lax.all_gather(mixer.astype(jnp.bfloat16), "tp", axis=1, tiled=True)
    glu_gate = jnp.dot(all_mixer, glu_weight, preferred_element_type=jnp.float32)
    gated = (mixer * jax.nn.sigmoid(glu_gate)).astype(jnp.bfloat16)
    all_gated = lax.all_gather(gated, "tp", axis=1, tiled=True)
    mixed = jnp.dot(all_gated, out_proj, preferred_element_type=jnp.float32)
    stream = (own_resid + mixed).astype(jnp.bfloat16)
    stream_f = stream.astype(jnp.float32)
    all_stream = lax.all_gather(stream, "tp", axis=1, tiled=True).astype(jnp.float32)
    inverse = lax.rsqrt(jnp.mean(all_stream * all_stream, axis=1, keepdims=True) + EPSILON)
    logits = jnp.dot(all_stream * ffn_gain, router, precision=high) * inverse
    payload = (all_stream * inverse * ffn_gain).astype(jnp.bfloat16)
    expert_count = router.shape[1]
    top_count = route_ids.shape[1]
    capacity = seq_rows * top_count // expert_count + 1
    expert_iota = jnp.arange(expert_count, dtype=jnp.int32)
    choose = (route_ids[:, :, None] == expert_iota).astype(jnp.float32)
    picked = jnp.sum(choose * logits[:, None, :], axis=2)
    expon = jnp.exp(picked)
    weights = expon / jnp.sum(expon, axis=1, keepdims=True)
    flat_route = route_ids.reshape(seq_rows * top_count)
    one_hot = (flat_route[:, None] == expert_iota).astype(jnp.int32)
    before = jnp.cumsum(one_hot, axis=0) - one_hot
    slot_ids = jnp.sum(before * one_hot, axis=1)
    target = flat_route * capacity + slot_ids
    slot_iota = jnp.arange(expert_count * capacity, dtype=jnp.int32)
    placing = jnp.any(slot_iota[:, None, None] == target.reshape(seq_rows, top_count)[None], axis=2)
    buffer = jnp.dot(placing.astype(jnp.bfloat16), payload, preferred_element_type=jnp.float32)
    buffer = buffer.astype(jnp.bfloat16).reshape(expert_count, capacity, payload.shape[1])
    local_experts = gate_weight.shape[0]
    received = lax.all_to_all(buffer, "ep", split_axis=0, concat_axis=0, tiled=True)
    items = received.shape[1]
    tokens = received.reshape(ep_size, local_experts, items, width)
    tokens = tokens.transpose(1, 0, 2, 3).reshape(local_experts, ep_size * items, width)
    gate_pre = jnp.einsum("esd,edf->esf", tokens, gate_weight, preferred_element_type=jnp.float32)
    up_pre = jnp.einsum("esd,edf->esf", tokens, up_weight, preferred_element_type=jnp.float32)
    gate_cl = jnp.minimum(gate_pre, LIMIT)
    up_cl = jnp.clip(up_pre, -LIMIT, LIMIT)
    active = ((up_cl + 1.0) * (gate_cl * jax.nn.sigmoid(ALPHA * gate_cl))).astype(jnp.bfloat16)
    partial_value = jnp.einsum(
        "esf,efd->esd", active, down_weight, preferred_element_type=jnp.float32
    ).astype(jnp.bfloat16)
    summed = lax.psum_scatter(
        partial_value.astype(jnp.float32).astype(jnp.bfloat16),
        "tp",
        scatter_dimension=2,
        tiled=True,
    )
    outgoing = summed.reshape(local_experts, ep_size, items, col_count)
    outgoing = outgoing.transpose(1, 0, 2, 3).reshape(ep_size * local_experts, items, col_count)
    returned = lax.all_to_all(outgoing, "ep", split_axis=0, concat_axis=0, tiled=True)
    flat_back = returned.reshape(expert_count * capacity, col_count)
    fetched = (
        jnp.take(flat_back, target, axis=0)
        .astype(jnp.float32)
        .reshape(seq_rows, top_count, col_count)
    )
    experts_sum = jnp.sum(weights[..., None] * fetched, axis=1)
    layer_out = (stream_f + experts_sum).astype(jnp.bfloat16)
    return (layer_out, state_re_new, state_im_new)


def erf(x):
    x = jnp.clip(x, -3.832506856900711, 3.832506856900711)
    y = x * x
    top = 0.00022905065861350646
    for coefficient in (
        0.0034082910107109506,
        0.050955695062380861,
        0.18520832239976145,
        1.128379143519084,
    ):
        top = top * y + coefficient
    bottom = -1.1791602954361697e-7
    for coefficient in (
        0.000023547966471313185,
        0.0010179625278914885,
        0.014070470171167667,
        0.11098505178285362,
        0.49746925110067538,
        1.0,
    ):
        bottom = bottom * y + coefficient
    return x * top / bottom


SENDS = ("g0", "g1", "g2", "g3", "place", "weight", "chips", "side", "relay", "twin", "back", "sum", "home")


def layer_kernel(
    sizes,
    resid_hbm,
    gain1_hbm,
    gain2_hbm,
    decay_hbm,
    freq_hbm,
    step_hbm,
    in_re_hbm,
    in_im_hbm,
    read_re_hbm,
    read_im_hbm,
    skip_hbm,
    router_hbm,
    route_hbm,
    sre_hbm,
    sim_hbm,
    proj_hbm,
    glu_hbm,
    outp_hbm,
    gate_hbm,
    up_hbm,
    down_hbm,
    out_ref,
    sre_out,
    sim_out,
    resid_ref,
    gains,
    poles,
    step_ref,
    in_maps,
    read_maps,
    skip_ref,
    router_ref,
    route_ref,
    state,
    proj,
    glu,
    outp,
    wg,
    wu,
    wd,
    res_all,
    mix_all,
    gated_all,
    logit_all,
    place_all,
    weight_all,
    pick,
    spill,
    tok,
    acc_g,
    acc_u,
    act,
    mine,
    sib_out,
    sib_in,
    summed,
    from_side,
    fwd_in,
    fwd_out,
    home_out,
    home_in,
    load_sem,
    send_sem,
    recv_sem,
):
    ep, tp, cap, rows = sizes
    f32, bf16 = jnp.float32, jnp.bfloat16
    me, t = lax.axis_index("ep"), lax.axis_index("tp")
    seqs, cols = resid_ref.shape
    width = cols * tp
    _, groups, states = poles.shape
    chans = skip_ref.shape[1]
    group_width = chans // groups
    chips = ep // 2
    pair = 2 * seqs
    half = seqs // 2
    last = (((1,), (1,)), ((), ()))

    def dot(a, b):
        return jnp.dot(a, b, preferred_element_type=f32)

    batches = {
        "resid": (resid_ref, [(resid_hbm, resid_ref)]),
        "route": (route_ref, [(route_hbm, route_ref)]),
        "step": (step_ref, [(step_hbm, step_ref)]),
        "poles": (poles, [(decay_hbm, poles.at[0]), (freq_hbm, poles.at[1])]),
        "in": (in_maps, [(in_re_hbm, in_maps.at[0]), (in_im_hbm, in_maps.at[1])]),
        "gains": (gains, [(gain1_hbm, gains.at[0]), (gain2_hbm, gains.at[1])]),
        "proj": (proj, [(proj_hbm, proj)]),
        "state": (state, [(sre_hbm, state.at[0]), (sim_hbm, state.at[1])]),
        "read": (read_maps, [(read_re_hbm, read_maps.at[0]), (read_im_hbm, read_maps.at[1])]),
        "skip": (skip_ref, [(skip_hbm, skip_ref)]),
        "glu": (glu, [(glu_hbm, glu)]),
        "outp": (outp, [(outp_hbm, outp)]),
        "router": (router_ref, [(router_hbm, router_ref)]),
        "gate": (wg, [(gate_hbm, wg)]),
        "up": (wu, [(up_hbm, wu)]),
        "down": (wd, [(down_hbm.at[:, j * cols : (j + 1) * cols], wd.at[j]) for j in range(tp)]),
    }
    names = list(batches)

    def absorb(ref, sem):
        pltpu.make_async_copy(ref, ref, sem).wait()

    def loaded(*wanted):
        for name in wanted:
            absorb(batches[name][0], load_sem.at[names.index(name)])

    for n, name in enumerate(names):
        for source, held in batches[name][1]:
            pltpu.make_async_copy(source, held, load_sem.at[n]).start()

    barrier = pltpu.get_barrier_semaphore()
    for k in range(1, tp):
        pl.semaphore_signal(barrier, inc=1, device_id=(me, (t + k) % tp), device_id_type=pl.DeviceIdType.MESH)
    for k in range(1, ep):
        pl.semaphore_signal(barrier, inc=1, device_id=((me + k) % ep, t), device_id_type=pl.DeviceIdType.MESH)
    pl.semaphore_wait(barrier, tp + ep - 2)

    arrivals = []

    def arrival(key):
        if key not in arrivals:
            arrivals.append(key)
        return recv_sem.at[arrivals.index(key)]

    def remote(source, target, peer, kind, key):
        pltpu.make_async_remote_copy(
            src_ref=source,
            dst_ref=target,
            send_sem=send_sem.at[SENDS.index(kind)],
            recv_sem=arrival(key),
            device_id=peer,
            device_id_type=pl.DeviceIdType.MESH,
        ).start()

    def flip(value, k):
        for bit in (1, 2, 4, 8, 16):
            if k & bit:
                value = value + bit - 2 * bit * ((value // bit) % 2)
        return value

    beside, across = flip(t, 1), flip(t, 2)
    opposite = flip(beside, 2)
    sibling = flip(me, 1)
    side_b, side_a, side_o, twin = (me, beside), (me, across), (me, opposite), (sibling, t)

    def gather(source, target, name):
        for k in (3, 1, 2):
            remote(source, target, (me, flip(t, k)), name, name)

    loaded("resid")
    gather(resid_ref, res_all.at[t], "g0")
    res_all[t] = resid_ref[...]

    loaded("route", "step", "poles", "in")
    square = (groups, groups)
    diagonal = lax.broadcasted_iota(jnp.int32, square, 0) == lax.broadcasted_iota(jnp.int32, square, 1)
    log_step = jnp.sum(
        jnp.where(diagonal, jnp.broadcast_to(step_ref[...], square), 0.0), axis=1, keepdims=True
    )
    step_size = jnp.exp(log_step)
    real_part, imag_part = -poles[0], poles[1]
    magnitude = jnp.exp(step_size * real_part)
    abar_re = magnitude * jnp.cos(step_size * imag_part)
    abar_im = magnitude * jnp.sin(step_size * imag_part)
    denom = real_part * real_part + imag_part * imag_part
    minus_one = abar_re - 1.0
    coef_re = ((minus_one * real_part + abar_im * imag_part) / denom)[:, None, :]
    coef_im = ((abar_im * real_part - minus_one * imag_part) / denom)[:, None, :]
    in_re, in_im = in_maps[0], in_maps[1]
    bb_re = (coef_re * in_re - coef_im * in_im).astype(bf16).reshape(chans, states)
    bb_im = (coef_re * in_im + coef_im * in_re).astype(bf16).reshape(chans, states)
    abar_re, abar_im = abar_re[None], abar_im[None]

    route = route_ref[...]
    iota_e = lax.broadcasted_iota(jnp.int32, (ep, seqs), 0)
    routed_t = jnp.zeros((ep, seqs), f32)
    for j in range(route.shape[0]):
        routed_t = routed_t + jnp.where(route[j : j + 1, :] == iota_e, 1.0, 0.0)
    row_i = lax.broadcasted_iota(jnp.int32, (seqs, seqs), 0)
    col_i = lax.broadcasted_iota(jnp.int32, (seqs, seqs), 1)
    earlier_t = dot(routed_t.astype(bf16), jnp.where(row_i < col_i, 1.0, 0.0).astype(bf16))
    place_all[0] = jnp.zeros(place_all.shape[1:], f32)
    place_all[0, :, 0:seqs] = jnp.where(routed_t > 0.5, earlier_t, -5000.0)
    for k in range(1, ep):
        remote(place_all.at[0], place_all.at[k], (flip(me, k), t), "place", "place")

    loaded("gains", "proj")
    absorb(res_all.at[0 : tp - 1], arrival("g0"))
    total = jnp.zeros((seqs, 1), f32)
    for j in range(tp):
        part = res_all[j].astype(f32)
        total = total + jnp.sum(part * part, axis=1, keepdims=True)
    scale = lax.rsqrt(total / width + EPSILON)
    mix = jnp.zeros((seqs, chans), f32)
    for j in range(tp):
        xnorm = (res_all[j].astype(f32) * scale * gains[0, j]).astype(bf16)
        mix = mix + dot(xnorm, proj[j * cols : (j + 1) * cols, :])
    mix_f = mix.astype(bf16).astype(f32)
    lane_c = lax.broadcasted_iota(jnp.int32, (seqs, groups, chans), 2)
    group_c = lax.broadcasted_iota(jnp.int32, (seqs, groups, chans), 1)
    first = group_c * group_width
    own = (lane_c >= first) & (lane_c < first + group_width)
    spread = jnp.where(own, jnp.broadcast_to(mix_f[:, None, :], own.shape), 0.0)
    spread = spread.astype(bf16).reshape(seqs * groups, chans)
    drive_re = dot(spread, bb_re).reshape(seqs, groups, states)
    drive_im = dot(spread, bb_im).reshape(seqs, groups, states)
    loaded("state", "read", "skip")
    old_re, old_im = state[0], state[1]
    new_re = abar_re * old_re - abar_im * old_im + drive_re
    new_im = abar_re * old_im + abar_im * old_re + drive_im
    sre_out[...] = new_re
    sim_out[...] = new_im
    flat = (seqs * groups, states)
    readout = lax.dot_general(
        new_re.reshape(flat).astype(bf16), read_maps[0].astype(bf16), last, preferred_element_type=f32
    ) - lax.dot_general(
        new_im.reshape(flat).astype(bf16), read_maps[1].astype(bf16), last, preferred_element_type=f32
    )
    readout = jnp.sum(jnp.where(own, readout.reshape(seqs, groups, chans), 0.0), axis=1)
    pre = readout + skip_ref[...] * mix_f
    mixer = 0.5 * pre * (1.0 + erf(pre * 0.7071067811865476))
    mix_all[t] = mixer.astype(bf16)
    gather(mix_all.at[t], mix_all.at[t], "g1")

    absorb(place_all.at[0 : ep - 1], arrival("place"))
    iota_r = lax.broadcasted_iota(jnp.int32, (rows, seqs), 0).astype(f32)
    iota_l = lax.broadcasted_iota(jnp.int32, (seqs, rows), 1).astype(f32)

    def slot_row(n, b):
        return place_all[2 * n + b, pl.ds(me, 1), 0:seqs] + float((n % 2 * 2 + b) * cap)

    for n in range(chips):
        for b in range(2):
            slots = slot_row(n, b)
            span = slice((n % 2 * 2 + b) * seqs, (n % 2 * 2 + b + 1) * seqs)
            pick[n // 2, :, span] = jnp.where(iota_r == slots, 1.0, 0.0).astype(bf16)
            down = jnp.sum(jnp.where(row_i == col_i, slots, 0.0), axis=1, keepdims=True)
            spill[n, b * seqs : (b + 1) * seqs, :] = jnp.where(iota_l == down, 1.0, 0.0).astype(bf16)

    loaded("glu")
    absorb(mix_all.at[0 : tp - 1], arrival("g1"))
    glu_gate = jnp.zeros((seqs, chans), f32)
    for j in range(tp):
        glu_gate = glu_gate + dot(mix_all[j], glu[j * chans : (j + 1) * chans, :])
    gated_all[t] = (mixer * jax.nn.sigmoid(glu_gate)).astype(bf16)
    gather(gated_all.at[t], gated_all.at[t], "g2")
    loaded("outp", "router")
    absorb(gated_all.at[0 : tp - 1], arrival("g2"))
    mixed = resid_ref[...].astype(f32)
    for j in range(tp):
        mixed = mixed + dot(gated_all[j], outp[j * chans : (j + 1) * chans, :])
    stream = mixed.astype(bf16)
    stream_f = stream.astype(f32)

    tok[0, t, 0:seqs, :] = stream
    top, bottom = pl.ds(0, half), pl.ds(half, half)

    def slab(n, j, b=0, cut=None):
        begin, size = (n % 2) * pair + b * seqs, seqs
        if cut is not None:
            begin, size = begin + cut * half, half
        return tok.at[n // 2, j, pl.ds(begin, size)]

    def to_twin(n, key, j):
        remote(slab(n, j, 0), slab(n, j, 1), twin, "twin", ("twin", n // 2, key))

    def spread_chips():
        for n in range(1, chips):
            remote(slab(0, t), slab(n, t), (flip(me, 2 * n), t), "chips", ("chips", n))

    def enter(n):
        if n:
            absorb(home_in.at[0], arrival(("chips", n)))
        block = slab(n, t)
        if n in direct_in:
            remote(block, block, side_o, "relay", ("corner", n))
        remote(block, block, side_b, "side", ("side", n))
        remote(block, block, side_a, "side", ("side", n))
        to_twin(n, "t", t)

    def relay(n):
        absorb(home_in.at[0:2], arrival(("side", n)))
        if n not in direct_in:
            first_b, second_a = slab(n, beside, 0, 0), slab(n, across, 0, 1)
            remote(first_b, first_b, side_a, "relay", ("corner", n))
            remote(second_a, second_a, side_b, "relay", ("corner", n))
        to_twin(n, "ba", beside)
        to_twin(n, "ba", across)

    def corner(n):
        absorb(home_in.at[0], arrival(("corner", n)))
        to_twin(n, "o", opposite)

    def logits():
        logit_all[t] = jnp.zeros(logit_all.shape[1:], f32)
        logit_all[t, 0:ep, 0:seqs] = lax.dot_general(
            router_ref[:, pl.ds(pl.multiple_of(t * cols, cols), cols)],
            stream_f * gains[1, t],
            last,
            precision=lax.Precision.HIGHEST,
            preferred_element_type=f32,
        )
        energy = jnp.sum(stream_f * stream_f, axis=1, keepdims=True)
        logit_all[t, ep : ep + 1, 0:seqs] = jnp.sum(
            jnp.where(row_i == col_i, energy, 0.0), axis=0, keepdims=True
        )
        gather(logit_all.at[t], logit_all.at[t], "g3")

    def weights():
        absorb(logit_all.at[0 : tp - 1], arrival("g3"))
        whole = logit_all[0]
        for j in range(1, tp):
            whole = whole + logit_all[j]
        whole = whole[:, 0:seqs]
        inverse = lax.rsqrt(whole[ep : ep + 1] / width + EPSILON)
        chosen = routed_t > 0.5
        expon = jnp.where(chosen, jnp.exp(jnp.where(chosen, whole[0:ep] * inverse, 0.0)), 0.0)
        weight_all[0] = jnp.zeros(weight_all.shape[1:], f32)
        weight_all[0, 0:ep, 0:seqs] = expon / jnp.sum(expon, axis=0, keepdims=True)
        weight_all[0, ep : ep + 1, 0:seqs] = inverse
        for k in range(1, ep):
            remote(weight_all.at[0], weight_all.at[k], (flip(me, k), t), "weight", "weight")

    def expert_in(h, key):
        places = {"t": [t], "ba": [beside, across], "o": [opposite]}[key]
        if (h, key) == (0, "t"):
            loaded("gate", "up")
        absorb(res_all.at[0 : 2 * len(places)], arrival(("twin", h, key)))
        total_g = total_u = None
        for j in places:
            scaled = (dot(pick[h], tok[h, j]) * gains[1, j]).astype(bf16)
            span = pl.ds(pl.multiple_of(j * cols, cols), cols)
            part_g, part_u = dot(scaled, wg[span, :]), dot(scaled, wu[span, :])
            total_g = part_g if total_g is None else total_g + part_g
            total_u = part_u if total_u is None else total_u + part_u
        if key == "t":
            acc_g[...] = total_g
            acc_u[...] = total_u
        else:
            acc_g[...] += total_g
            acc_u[...] += total_u

    def activate(h):
        if h == 0:
            absorb(weight_all.at[0 : ep - 1], arrival("weight"))
        norm = jnp.zeros((rows, 1), f32)
        share = jnp.zeros((rows, 1), f32)
        for n in (2 * h, 2 * h + 1):
            for b in range(2):
                match = iota_r == slot_row(n, b)
                inverse = weight_all[2 * n + b, ep : ep + 1, 0:seqs]
                weight = weight_all[2 * n + b, pl.ds(me, 1), 0:seqs]
                norm = norm + jnp.sum(jnp.where(match, inverse, 0.0), axis=1, keepdims=True)
                share = share + jnp.sum(jnp.where(match, weight, 0.0), axis=1, keepdims=True)
        gate_cl = jnp.minimum(acc_g[...] * norm, LIMIT)
        up_cl = jnp.clip(acc_u[...] * norm, -LIMIT, LIMIT)
        act[h] = (((up_cl + 1.0) * share) * (gate_cl * jax.nn.sigmoid(ALPHA * gate_cl))).astype(bf16)

    def expert_out(n):
        if n == outs[0]:
            loaded("down")
        spread_act = dot(spill[n], act[n // 2]).astype(bf16)
        order = (opposite, beside, across, t)
        for j in order:
            value = dot(spread_act, wd[j])
            sib_out[n, j] = value[seqs:].astype(bf16)
            mine[n, j] = value[:seqs]
        remote(sib_out.at[n], sib_in.at[n], twin, "back", ("back", n))

    def reduce_chip(n):
        absorb(sib_in.at[n], arrival(("back", n)))
        for j in (opposite, beside, across):
            both = mine[n, j] + sib_in[n, j].astype(f32)
            mine[n, j] = both
            summed[n, j] = both.astype(bf16)
        if n in direct_out:
            remote(summed.at[n, opposite], from_side.at[n, 2], side_o, "sum", ("mine", n))
            remote(summed.at[n, beside], from_side.at[n, 0], side_b, "sum", ("mine", n))
            remote(summed.at[n, across], from_side.at[n, 1], side_a, "sum", ("mine", n))
            return
        remote(summed.at[n, opposite, top], fwd_in.at[n, 0], side_b, "sum", ("fwd", n))
        remote(summed.at[n, opposite, bottom], fwd_in.at[n, 1], side_a, "sum", ("fwd", n))
        remote(summed.at[n, beside, top], from_side.at[n, 0, top], side_b, "sum", ("mine", n))
        remote(summed.at[n, across, bottom], from_side.at[n, 1, bottom], side_a, "sum", ("mine", n))

    def reduce_relay(n):
        if n in direct_out:
            return
        absorb(fwd_in.at[n], arrival(("fwd", n)))
        fwd_out[n, 0] = (mine[n, across, 0:half] + fwd_in[n, 0].astype(f32)).astype(bf16)
        fwd_out[n, 1] = (mine[n, beside, half:] + fwd_in[n, 1].astype(f32)).astype(bf16)
        remote(fwd_out.at[n, 0], from_side.at[n, 1, top], side_a, "sum", ("mine", n))
        remote(fwd_out.at[n, 1], from_side.at[n, 0, bottom], side_b, "sum", ("mine", n))

    def go_home(n):
        value = mine[n, t] + sib_in[n, t].astype(f32)
        count = 3 if n in direct_out else 2
        absorb(from_side.at[n, 0:count], arrival(("mine", n)))
        for k in range(count):
            value = value + from_side[n, k].astype(f32)
        if n:
            home_out[n] = value.astype(bf16)
            remote(home_out.at[n], home_in.at[n], (flip(me, 2 * n), t), "home", "home")
        else:
            mine[n, t] = value

    def finish():
        result = stream_f + mine[0, t]
        absorb(home_in.at[0 : chips - 1], arrival("home"))
        for n in range(1, chips):
            result = result + home_in[n].astype(f32)
        out_ref[...] = result.astype(bf16)

    direct_in, direct_out = (), ()
    outs = (1, 0, 3, 2)
    plan = [
        (spread_chips,), (enter, 0), (logits,),
        (relay, 0), (enter, 1), (weights,), (enter, 2), (corner, 0), (relay, 1),
        (expert_in, 0, "t"), (enter, 3), (relay, 2), (corner, 1), (expert_in, 0, "ba"),
        (expert_in, 0, "o"), (relay, 3), (corner, 2), (activate, 0), (expert_out, 1), (expert_out, 0), (corner, 3),
        (expert_in, 1, "t"), (reduce_chip, 1), (expert_in, 1, "ba"), (reduce_chip, 0), (expert_in, 1, "o"), (activate, 1),
        (reduce_relay, 1), (expert_out, 3), (reduce_relay, 0), (expert_out, 2), (go_home, 1), (reduce_chip, 3), (go_home, 0), (reduce_chip, 2),
        (reduce_relay, 3), (reduce_relay, 2), (go_home, 3), (go_home, 2),
        (finish,),
    ]
    for step in plan:
        step[0](*step[1:])
    spent = {
        "g0": res_all.at[0 : tp - 1],
        "g1": mix_all.at[0 : tp - 1],
        "g2": gated_all.at[0 : tp - 1],
        "g3": logit_all.at[0 : tp - 1],
        "place": place_all.at[0 : ep - 1],
        "weight": weight_all.at[0 : ep - 1],
        "chips": home_in.at[0 : chips - 1],
        "side": tok.at[0, 0 : chips // 2],
        "relay": tok.at[0, 0],
        "twin": tok.at[0, 0:chips],
        "back": sib_in,
        "home": home_in.at[0 : chips - 1],
    }
    for kind, ref in spent.items():
        absorb(ref, send_sem.at[SENDS.index(kind)])
    absorb(sib_in.at[:, 0:3], send_sem.at[SENDS.index("sum")])


def finish_kernel(a_in, b_in, c_in, a_out, b_out, c_out, sems):
    writes = [
        pltpu.make_async_copy(held, target, sems.at[n])
        for n, (held, target) in enumerate(((a_in, a_out), (b_in, b_out), (c_in, c_out)))
    ]
    for write in writes:
        write.start()
    for write in writes:
        write.wait()


def dispatch(*args):
    (
        residual, state_re, state_im, mix_gain, proj_in, decay_rate, frequency, log_step,
        input_re, input_im, read_re, read_im, skip_gain, glu_weight, out_proj, ffn_gain,
        router, gate_weight, up_weight, down_weight, route_ids,
    ) = args
    ep, tp = lax.axis_size("ep"), lax.axis_size("tp")
    seqs, cols = residual.shape
    groups, states = decay_rate.shape
    chans = skip_gain.shape[0]
    rough = groups % 16 or chans % 128 or cols % 128 or seqs % 32 or seqs > 128
    if gate_weight.shape[0] != 1 or tp != 4 or ep != 8 or rough:
        return per_device(*args)
    top = route_ids.shape[1]
    cap = seqs * top // router.shape[1] + 1
    rows = -(-4 * cap // 16) * 16
    hidden = gate_weight.shape[2]
    width = mix_gain.shape[0]
    chips = ep // 2
    halves = chips // 2
    bf16, f32 = jnp.bfloat16, jnp.float32
    hbm, vmem = pl.BlockSpec(memory_space=pltpu.HBM), pl.BlockSpec(memory_space=pltpu.VMEM)
    state_shape = (seqs, groups, states)
    blocks = (chips, tp, seqs, cols)
    out = pl.pallas_call(
        functools.partial(layer_kernel, (ep, tp, cap, rows)),
        out_shape=(
            pltpu.VMEM((seqs, cols), bf16),
            pltpu.VMEM(state_shape, f32),
            pltpu.VMEM(state_shape, f32),
        ),
        in_specs=[hbm] * 21,
        out_specs=(vmem, vmem, vmem),
        scratch_shapes=[
            pltpu.VMEM((seqs, cols), bf16),
            pltpu.VMEM((2, tp, 1, cols), f32),
            pltpu.VMEM((2, groups, states), f32),
            pltpu.VMEM((1, groups), f32),
            pltpu.VMEM((2, groups, chans // groups, states), f32),
            pltpu.VMEM((2, chans, states), f32),
            pltpu.VMEM((1, chans), f32),
            pltpu.VMEM((ep, width), f32),
            pltpu.VMEM((top, seqs), jnp.int32),
            pltpu.VMEM((2,) + state_shape, f32),
            pltpu.VMEM(proj_in.shape, bf16),
            pltpu.VMEM(glu_weight.shape, bf16),
            pltpu.VMEM(out_proj.shape, bf16),
            pltpu.VMEM(gate_weight.shape[1:], bf16),
            pltpu.VMEM(up_weight.shape[1:], bf16),
            pltpu.VMEM((tp, hidden, cols), bf16),
            pltpu.VMEM((tp, seqs, cols), bf16),
            pltpu.VMEM((tp, seqs, chans), bf16),
            pltpu.VMEM((tp, seqs, chans), bf16),
            pltpu.VMEM((tp, 2 * ep, 128), f32),
            pltpu.VMEM((ep, ep, 128), f32),
            pltpu.VMEM((ep, 2 * ep, 128), f32),
            pltpu.VMEM((halves, rows, 4 * seqs), bf16),
            pltpu.VMEM((chips, 2 * seqs, rows), bf16),
            pltpu.VMEM((halves, tp, 4 * seqs, cols), bf16),
            pltpu.VMEM((rows, hidden), f32),
            pltpu.VMEM((rows, hidden), f32),
            pltpu.VMEM((halves, rows, hidden), bf16),
            pltpu.VMEM(blocks, f32),
            pltpu.VMEM(blocks, bf16),
            pltpu.VMEM(blocks, bf16),
            pltpu.VMEM(blocks, bf16),
            pltpu.VMEM((chips, 3, seqs, cols), bf16),
            pltpu.VMEM((chips, 2, seqs // 2, cols), bf16),
            pltpu.VMEM((chips, 2, seqs // 2, cols), bf16),
            pltpu.VMEM((chips, seqs, cols), bf16),
            pltpu.VMEM((chips, seqs, cols), bf16),
            pltpu.SemaphoreType.DMA((16,)),
            pltpu.SemaphoreType.DMA((len(SENDS),)),
            pltpu.SemaphoreType.DMA((44,)),
        ],
        compiler_params=pltpu.CompilerParams(
            collective_id=0, has_side_effects=True, vmem_limit_bytes=48 * 1024 * 1024
        ),
        name="layer",
    )(*(pltpu.with_memory_space_constraint(part, pltpu.HBM) for part in (
        residual,
        mix_gain.reshape(tp, 1, cols),
        ffn_gain.reshape(tp, 1, cols),
        decay_rate,
        frequency,
        log_step.reshape(1, groups),
        input_re.transpose(0, 2, 1),
        input_im.transpose(0, 2, 1),
        read_re.reshape(chans, states),
        read_im.reshape(chans, states),
        skip_gain.reshape(1, chans),
        router.T,
        route_ids.T,
        state_re,
        state_im,
        proj_in,
        glu_weight,
        out_proj,
        gate_weight.reshape(gate_weight.shape[1:]),
        up_weight.reshape(up_weight.shape[1:]),
        down_weight.reshape(down_weight.shape[1:]),
    )))
    return pl.pallas_call(
        finish_kernel,
        out_shape=tuple(jax.ShapeDtypeStruct(part.shape, part.dtype) for part in out),
        in_specs=[vmem] * 3,
        out_specs=(hbm,) * 3,
        scratch_shapes=[pltpu.SemaphoreType.DMA((3,))],
        compiler_params=pltpu.CompilerParams(vmem_limit_bytes=8 * 1024 * 1024),
        name="finish",
    )(*out)


def solution(mesh):
    in_specs = (
        P("ep", "tp"),
        P("ep", "tp", None),
        P("ep", "tp", None),
        P(),
        P(None, "tp"),
        P("tp", None),
        P("tp", None),
        P("tp"),
        P("tp", None, None),
        P("tp", None, None),
        P("tp", None, None),
        P("tp", None, None),
        P("tp"),
        P(None, "tp"),
        P(None, "tp"),
        P(),
        P(),
        P("ep", None, "tp"),
        P("ep", None, "tp"),
        P("ep", "tp", None),
        P("ep", None),
    )
    out_specs = (P("ep", "tp"), P("ep", "tp", None), P("ep", "tp", None))
    return jax.shard_map(
        dispatch, mesh=mesh, in_specs=in_specs, out_specs=out_specs, check_vma=False
    )
```

```python
import functools

import jax
import jax.numpy as jnp
from jax import lax
from jax.experimental import pallas as pl
from jax.experimental.pallas import tpu as pltpu
from jax.sharding import PartitionSpec as P

EPSILON = 1e-05
LIMIT = 7.0
ALPHA = 1.702


def discretise(decay_rate, frequency, log_step, input_re, input_im):
    real_part = -decay_rate
    step_size = jnp.exp(log_step)[:, None]
    magnitude = jnp.exp(step_size * real_part)
    abar_re = magnitude * jnp.cos(step_size * frequency)
    abar_im = magnitude * jnp.sin(step_size * frequency)
    denom = real_part * real_part + frequency * frequency
    minus_one = abar_re - 1.0
    coef_re = (minus_one * real_part + abar_im * frequency) / denom
    coef_im = (abar_im * real_part - minus_one * frequency) / denom
    bbar_re = coef_re[..., None] * input_re - coef_im[..., None] * input_im
    bbar_im = coef_re[..., None] * input_im + coef_im[..., None] * input_re
    return (abar_re, abar_im, bbar_re, bbar_im)


def per_device(
    residual,
    state_re,
    state_im,
    mix_gain,
    proj_in,
    decay_rate,
    frequency,
    log_step,
    input_re,
    input_im,
    read_re,
    read_im,
    skip_gain,
    glu_weight,
    out_proj,
    ffn_gain,
    router,
    gate_weight,
    up_weight,
    down_weight,
    route_ids,
):
    high = lax.Precision.HIGHEST
    seq_rows = residual.shape[0]
    col_count = residual.shape[1]
    width = mix_gain.shape[0]
    ep_size = lax.axis_size("ep")
    own_resid = residual.astype(jnp.float32)
    full_resid = lax.all_gather(residual, "tp", axis=1, tiled=True).astype(jnp.float32)
    scale_one = lax.rsqrt(jnp.mean(full_resid * full_resid, axis=1, keepdims=True) + EPSILON)
    xnorm = (full_resid * scale_one * mix_gain).astype(jnp.bfloat16)
    mix_in = jnp.dot(xnorm, proj_in, preferred_element_type=jnp.float32).astype(jnp.bfloat16)
    mix_f = mix_in.astype(jnp.float32)
    group_count = decay_rate.shape[0]
    group_width = input_re.shape[2]
    grouped = mix_f.reshape(seq_rows, group_count, group_width)
    abar_re, abar_im, bbar_re, bbar_im = discretise(
        decay_rate, frequency, log_step, input_re, input_im
    )
    drive_re = jnp.einsum("sgc,gnc->sgn", grouped, bbar_re, precision=high)
    drive_im = jnp.einsum("sgc,gnc->sgn", grouped, bbar_im, precision=high)
    state_re_new = abar_re * state_re - abar_im * state_im + drive_re
    state_im_new = abar_re * state_im + abar_im * state_re + drive_im
    readout = jnp.einsum("sgn,gcn->sgc", state_re_new, read_re, precision=high) - jnp.einsum(
        "sgn,gcn->sgc", state_im_new, read_im, precision=high
    )
    mixer = jax.nn.gelu(
        readout.reshape(seq_rows, group_count * group_width) + skip_gain * mix_f, approximate=False
    )
    all_mixer = lax.all_gather(mixer.astype(jnp.bfloat16), "tp", axis=1, tiled=True)
    glu_gate = jnp.dot(all_mixer, glu_weight, preferred_element_type=jnp.float32)
    gated = (mixer * jax.nn.sigmoid(glu_gate)).astype(jnp.bfloat16)
    all_gated = lax.all_gather(gated, "tp", axis=1, tiled=True)
    mixed = jnp.dot(all_gated, out_proj, preferred_element_type=jnp.float32)
    stream = (own_resid + mixed).astype(jnp.bfloat16)
    stream_f = stream.astype(jnp.float32)
    all_stream = lax.all_gather(stream, "tp", axis=1, tiled=True).astype(jnp.float32)
    inverse = lax.rsqrt(jnp.mean(all_stream * all_stream, axis=1, keepdims=True) + EPSILON)
    logits = jnp.dot(all_stream * ffn_gain, router, precision=high) * inverse
    payload = (all_stream * inverse * ffn_gain).astype(jnp.bfloat16)
    expert_count = router.shape[1]
    top_count = route_ids.shape[1]
    capacity = seq_rows * top_count // expert_count + 1
    expert_iota = jnp.arange(expert_count, dtype=jnp.int32)
    choose = (route_ids[:, :, None] == expert_iota).astype(jnp.float32)
    picked = jnp.sum(choose * logits[:, None, :], axis=2)
    expon = jnp.exp(picked)
    weights = expon / jnp.sum(expon, axis=1, keepdims=True)
    flat_route = route_ids.reshape(seq_rows * top_count)
    one_hot = (flat_route[:, None] == expert_iota).astype(jnp.int32)
    before = jnp.cumsum(one_hot, axis=0) - one_hot
    slot_ids = jnp.sum(before * one_hot, axis=1)
    target = flat_route * capacity + slot_ids
    slot_iota = jnp.arange(expert_count * capacity, dtype=jnp.int32)
    placing = jnp.any(slot_iota[:, None, None] == target.reshape(seq_rows, top_count)[None], axis=2)
    buffer = jnp.dot(placing.astype(jnp.bfloat16), payload, preferred_element_type=jnp.float32)
    buffer = buffer.astype(jnp.bfloat16).reshape(expert_count, capacity, payload.shape[1])
    local_experts = gate_weight.shape[0]
    received = lax.all_to_all(buffer, "ep", split_axis=0, concat_axis=0, tiled=True)
    items = received.shape[1]
    tokens = received.reshape(ep_size, local_experts, items, width)
    tokens = tokens.transpose(1, 0, 2, 3).reshape(local_experts, ep_size * items, width)
    gate_pre = jnp.einsum("esd,edf->esf", tokens, gate_weight, preferred_element_type=jnp.float32)
    up_pre = jnp.einsum("esd,edf->esf", tokens, up_weight, preferred_element_type=jnp.float32)
    gate_cl = jnp.minimum(gate_pre, LIMIT)
    up_cl = jnp.clip(up_pre, -LIMIT, LIMIT)
    active = ((up_cl + 1.0) * (gate_cl * jax.nn.sigmoid(ALPHA * gate_cl))).astype(jnp.bfloat16)
    partial_value = jnp.einsum(
        "esf,efd->esd", active, down_weight, preferred_element_type=jnp.float32
    ).astype(jnp.bfloat16)
    summed = lax.psum_scatter(
        partial_value.astype(jnp.float32).astype(jnp.bfloat16),
        "tp",
        scatter_dimension=2,
        tiled=True,
    )
    outgoing = summed.reshape(local_experts, ep_size, items, col_count)
    outgoing = outgoing.transpose(1, 0, 2, 3).reshape(ep_size * local_experts, items, col_count)
    returned = lax.all_to_all(outgoing, "ep", split_axis=0, concat_axis=0, tiled=True)
    flat_back = returned.reshape(expert_count * capacity, col_count)
    fetched = (
        jnp.take(flat_back, target, axis=0)
        .astype(jnp.float32)
        .reshape(seq_rows, top_count, col_count)
    )
    experts_sum = jnp.sum(weights[..., None] * fetched, axis=1)
    layer_out = (stream_f + experts_sum).astype(jnp.bfloat16)
    return (layer_out, state_re_new, state_im_new)


def erf(x):
    x = jnp.clip(x, -3.832506856900711, 3.832506856900711)
    y = x * x
    top = 0.00022905065861350646
    for coefficient in (
        0.0034082910107109506,
        0.050955695062380861,
        0.18520832239976145,
        1.128379143519084,
    ):
        top = top * y + coefficient
    bottom = -1.1791602954361697e-7
    for coefficient in (
        0.000023547966471313185,
        0.0010179625278914885,
        0.014070470171167667,
        0.11098505178285362,
        0.49746925110067538,
        1.0,
    ):
        bottom = bottom * y + coefficient
    return x * top / bottom


SENDS = ("g0", "g1", "g2", "g3", "weight", "chips", "side", "relay", "twin", "back", "sum", "home")


def layer_kernel(
    sizes,
    resid_hbm,
    gain1_hbm,
    gain2_hbm,
    decay_hbm,
    freq_hbm,
    step_hbm,
    in_re_hbm,
    in_im_hbm,
    read_re_hbm,
    read_im_hbm,
    skip_hbm,
    router_hbm,
    route_hbm,
    sre_hbm,
    sim_hbm,
    proj_hbm,
    glu_hbm,
    outp_hbm,
    gate_hbm,
    up_hbm,
    down_hbm,
    out_ref,
    sre_out,
    sim_out,
    resid_ref,
    gains,
    poles,
    step_ref,
    in_maps,
    read_maps,
    skip_ref,
    router_ref,
    route_ref,
    state,
    proj,
    glu,
    outp,
    wgu,
    wd,
    res_all,
    mix_all,
    gated_all,
    logit_all,
    weight_all,
    tok,
    ready,
    acc,
    act,
    mine,
    sib_out,
    sib_in,
    summed,
    from_side,
    fwd_in,
    fwd_out,
    home_out,
    home_in,
    load_sem,
    send_sem,
    recv_sem,
):
    ep, tp = sizes
    rows = 2 * resid_ref.shape[0]
    f32, bf16 = jnp.float32, jnp.bfloat16
    me, t = lax.axis_index("ep"), lax.axis_index("tp")
    seqs, cols = resid_ref.shape
    width = cols * tp
    _, groups, states = poles.shape
    chans = skip_ref.shape[1]
    group_width = chans // groups
    chips = ep // 2
    half = seqs // 2
    hidden = wd.shape[1]
    last = (((1,), (1,)), ((), ()))

    def dot(a, b):
        return jnp.dot(a, b, preferred_element_type=f32)

    batches = {
        "resid": (resid_ref, [(resid_hbm, resid_ref)]),
        "route": (route_ref, [(route_hbm, route_ref)]),
        "step": (step_ref, [(step_hbm, step_ref)]),
        "poles": (poles, [(decay_hbm, poles.at[0]), (freq_hbm, poles.at[1])]),
        "in": (in_maps, [(in_re_hbm, in_maps.at[0]), (in_im_hbm, in_maps.at[1])]),
        "gains": (gains, [(gain1_hbm, gains.at[0]), (gain2_hbm, gains.at[1])]),
        "proj": (proj, [(proj_hbm, proj)]),
        "state": (state, [(sre_hbm, state.at[0]), (sim_hbm, state.at[1])]),
        "read": (read_maps, [(read_re_hbm, read_maps.at[0]), (read_im_hbm, read_maps.at[1])]),
        "skip": (skip_ref, [(skip_hbm, skip_ref)]),
        "glu": (glu, [(glu_hbm, glu)]),
        "outp": (outp, [(outp_hbm, outp)]),
        "router": (router_ref, [(router_hbm, router_ref)]),
        "experts": (wgu, [(gate_hbm, wgu.at[:, 0:hidden]), (up_hbm, wgu.at[:, hidden : 2 * hidden])]),
        "down": (wd, [(down_hbm.at[:, j * cols : (j + 1) * cols], wd.at[j]) for j in range(tp)]),
    }
    names = list(batches)

    def absorb(ref, sem):
        pltpu.make_async_copy(ref, ref, sem).wait()

    def loaded(*wanted):
        for name in wanted:
            absorb(batches[name][0], load_sem.at[names.index(name)])

    for n, name in enumerate(names):
        for source, held in batches[name][1]:
            pltpu.make_async_copy(source, held, load_sem.at[n]).start()

    barrier = pltpu.get_barrier_semaphore()
    for k in range(1, tp):
        pl.semaphore_signal(barrier, inc=1, device_id=(me, (t + k) % tp), device_id_type=pl.DeviceIdType.MESH)
    for k in range(1, ep):
        pl.semaphore_signal(barrier, inc=1, device_id=((me + k) % ep, t), device_id_type=pl.DeviceIdType.MESH)
    pl.semaphore_wait(barrier, tp + ep - 2)

    arrivals = []

    def arrival(key):
        if key not in arrivals:
            arrivals.append(key)
        return recv_sem.at[arrivals.index(key)]

    def remote(source, target, peer, kind, key):
        pltpu.make_async_remote_copy(
            src_ref=source,
            dst_ref=target,
            send_sem=send_sem.at[SENDS.index(kind)],
            recv_sem=arrival(key),
            device_id=peer,
            device_id_type=pl.DeviceIdType.MESH,
        ).start()

    def flip(value, k):
        for bit in (1, 2, 4, 8, 16):
            if k & bit:
                value = value + bit - 2 * bit * ((value // bit) % 2)
        return value

    beside, across = flip(t, 1), flip(t, 2)
    opposite = flip(beside, 2)
    sibling = flip(me, 1)
    side_b, side_a, side_o, twin = (me, beside), (me, across), (me, opposite), (sibling, t)

    def gather(source, target, name):
        for k in (3, 1, 2):
            remote(source, target, (me, flip(t, k)), name, name)

    loaded("resid")
    gather(resid_ref, res_all.at[t], "g0")
    res_all[t] = resid_ref[...]

    loaded("route", "step", "poles", "in")
    square = (groups, groups)
    diagonal = lax.broadcasted_iota(jnp.int32, square, 0) == lax.broadcasted_iota(jnp.int32, square, 1)
    log_step = jnp.sum(
        jnp.where(diagonal, jnp.broadcast_to(step_ref[...], square), 0.0), axis=1, keepdims=True
    )
    step_size = jnp.exp(log_step)
    real_part, imag_part = -poles[0], poles[1]
    magnitude = jnp.exp(step_size * real_part)
    abar_re = magnitude * jnp.cos(step_size * imag_part)
    abar_im = magnitude * jnp.sin(step_size * imag_part)
    denom = real_part * real_part + imag_part * imag_part
    minus_one = abar_re - 1.0
    coef_re = ((minus_one * real_part + abar_im * imag_part) / denom)[:, None, :]
    coef_im = ((abar_im * real_part - minus_one * imag_part) / denom)[:, None, :]
    in_re, in_im = in_maps[0], in_maps[1]
    bb_re = (coef_re * in_re - coef_im * in_im).astype(bf16).reshape(chans, states)
    bb_im = (coef_re * in_im + coef_im * in_re).astype(bf16).reshape(chans, states)
    abar_re, abar_im = abar_re[None], abar_im[None]

    route = route_ref[...]
    iota_e = lax.broadcasted_iota(jnp.int32, (ep, seqs), 0)
    routed_t = jnp.zeros((ep, seqs), f32)
    for j in range(route.shape[0]):
        routed_t = routed_t + jnp.where(route[j : j + 1, :] == iota_e, 1.0, 0.0)
    row_i = lax.broadcasted_iota(jnp.int32, (seqs, seqs), 0)
    col_i = lax.broadcasted_iota(jnp.int32, (seqs, seqs), 1)

    loaded("gains", "proj")
    absorb(res_all.at[0 : tp - 1], arrival("g0"))
    total = jnp.zeros((seqs, 1), f32)
    for j in range(tp):
        part = res_all[j].astype(f32)
        total = total + jnp.sum(part * part, axis=1, keepdims=True)
    scale = lax.rsqrt(total / width + EPSILON)
    mix = jnp.zeros((seqs, chans), f32)
    for j in range(tp):
        xnorm = (res_all[j].astype(f32) * scale * gains[0, j]).astype(bf16)
        mix = mix + dot(xnorm, proj[j * cols : (j + 1) * cols, :])
    mix_f = mix.astype(bf16).astype(f32)
    lane_c = lax.broadcasted_iota(jnp.int32, (seqs, groups, chans), 2)
    group_c = lax.broadcasted_iota(jnp.int32, (seqs, groups, chans), 1)
    first = group_c * group_width
    own = (lane_c >= first) & (lane_c < first + group_width)
    spread = jnp.where(own, jnp.broadcast_to(mix_f[:, None, :], own.shape), 0.0)
    spread = spread.astype(bf16).reshape(seqs * groups, chans)
    drive_re = dot(spread, bb_re).reshape(seqs, groups, states)
    drive_im = dot(spread, bb_im).reshape(seqs, groups, states)
    loaded("state", "read", "skip")
    old_re, old_im = state[0], state[1]
    new_re = abar_re * old_re - abar_im * old_im + drive_re
    new_im = abar_re * old_im + abar_im * old_re + drive_im
    sre_out[...] = new_re
    sim_out[...] = new_im
    flat = (seqs * groups, states)
    readout = lax.dot_general(
        new_re.reshape(flat).astype(bf16), read_maps[0].astype(bf16), last, preferred_element_type=f32
    ) - lax.dot_general(
        new_im.reshape(flat).astype(bf16), read_maps[1].astype(bf16), last, preferred_element_type=f32
    )
    readout = jnp.sum(jnp.where(own, readout.reshape(seqs, groups, chans), 0.0), axis=1)
    pre = readout + skip_ref[...] * mix_f
    mixer = 0.5 * pre * (1.0 + erf(pre * 0.7071067811865476))
    mix_all[t] = mixer.astype(bf16)
    gather(mix_all.at[t], mix_all.at[t], "g1")

    loaded("glu")
    absorb(mix_all.at[0 : tp - 1], arrival("g1"))
    glu_gate = jnp.zeros((seqs, chans), f32)
    for j in range(tp):
        glu_gate = glu_gate + dot(mix_all[j], glu[j * chans : (j + 1) * chans, :])
    gated_all[t] = (mixer * jax.nn.sigmoid(glu_gate)).astype(bf16)
    gather(gated_all.at[t], gated_all.at[t], "g2")
    loaded("outp", "router")
    absorb(gated_all.at[0 : tp - 1], arrival("g2"))
    mixed = resid_ref[...].astype(f32)
    for j in range(tp):
        mixed = mixed + dot(gated_all[j], outp[j * chans : (j + 1) * chans, :])
    stream = mixed.astype(bf16)
    stream_f = stream.astype(f32)

    tok[0, t, 0:seqs, :] = stream
    top, bottom = pl.ds(0, half), pl.ds(half, half)

    def slab(n, j, b=0, cut=None):
        begin, size = b * seqs, seqs
        if cut is not None:
            begin, size = begin + cut * half, half
        return tok.at[n, j, pl.ds(begin, size)]

    def to_twin(n, key, j):
        remote(slab(n, j, 0), slab(n, j, 1), twin, "twin", ("twin", n, key))

    def spread_chips():
        for n in range(1, chips):
            remote(slab(0, t), slab(n, t), (flip(me, 2 * n), t), "chips", ("chips", n))

    def enter(n):
        if n:
            absorb(home_in.at[0], arrival(("chips", n)))
        block = slab(n, t)
        if n in direct_in:
            remote(block, block, side_o, "relay", ("corner", n))
        remote(block, block, side_b, "side", ("side", n))
        remote(block, block, side_a, "side", ("side", n))
        to_twin(n, "t", t)

    def relay(n):
        absorb(home_in.at[0:2], arrival(("side", n)))
        if n not in direct_in:
            first_b, second_a = slab(n, beside, 0, 0), slab(n, across, 0, 1)
            remote(first_b, first_b, side_a, "relay", ("corner", n))
            remote(second_a, second_a, side_b, "relay", ("corner", n))
        to_twin(n, "ba", beside)
        to_twin(n, "ba", across)

    def corner(n):
        absorb(home_in.at[0], arrival(("corner", n)))
        to_twin(n, "o", opposite)

    def logits():
        logit_all[t] = jnp.zeros(logit_all.shape[1:], f32)
        logit_all[t, 0:ep, 0:seqs] = lax.dot_general(
            router_ref[:, pl.ds(pl.multiple_of(t * cols, cols), cols)],
            stream_f * gains[1, t],
            last,
            precision=lax.Precision.HIGHEST,
            preferred_element_type=f32,
        )
        energy = jnp.sum(stream_f * stream_f, axis=1, keepdims=True)
        logit_all[t, ep : ep + 1, 0:seqs] = jnp.sum(
            jnp.where(row_i == col_i, energy, 0.0), axis=0, keepdims=True
        )
        gather(logit_all.at[t], logit_all.at[t], "g3")

    def weights():
        absorb(logit_all.at[0 : tp - 1], arrival("g3"))
        whole = logit_all[0]
        for j in range(1, tp):
            whole = whole + logit_all[j]
        whole = whole[:, 0:seqs]
        inverse = lax.rsqrt(whole[ep : ep + 1] / width + EPSILON)
        chosen = routed_t > 0.5
        expon = jnp.where(chosen, jnp.exp(jnp.where(chosen, whole[0:ep] * inverse, 0.0)), 0.0)
        weight_all[0] = jnp.zeros(weight_all.shape[1:], f32)
        weight_all[0, 0:ep, 0:seqs] = expon / jnp.sum(expon, axis=0, keepdims=True)
        weight_all[0, ep : ep + 1, 0:seqs] = inverse
        for k in range(1, ep):
            remote(weight_all.at[0], weight_all.at[k], (flip(me, k), t), "weight", "weight")

    def scale_in(n, key):
        for name, places in (("t", [t]), ("ba", [beside, across]), ("o", [opposite])):
            if name not in key:
                continue
            absorb(res_all.at[0 : len(places)], arrival(("twin", n, name)))
            for j in places:
                span = pl.ds(pl.multiple_of(j * cols, cols), cols)
                ready[n, :, span] = (tok[n, j].astype(f32) * gains[1, j]).astype(bf16)

    def expert_in(n):
        if n == outs[0]:
            loaded("experts")
        acc[...] = dot(ready[n], wgu[...])

    def column(line):
        return jnp.sum(jnp.where(row_i == col_i, line, 0.0), axis=1, keepdims=True)

    def activate(n):
        if n == outs[0]:
            absorb(weight_all.at[0 : ep - 1], arrival("weight"))
        for b in range(2):
            lines = slice(b * seqs, (b + 1) * seqs)
            norm = column(weight_all[2 * n + b, ep : ep + 1, 0:seqs])
            share = column(weight_all[2 * n + b, pl.ds(me, 1), 0:seqs])
            gate_cl = jnp.minimum(acc[lines, 0:hidden] * norm, LIMIT)
            up_cl = jnp.clip(acc[lines, hidden:] * norm, -LIMIT, LIMIT)
            act[n, lines] = (((up_cl + 1.0) * share) * (gate_cl * jax.nn.sigmoid(ALPHA * gate_cl))).astype(bf16)

    def expert_out(n):
        if n == outs[0]:
            loaded("down")
        for number, j in enumerate((opposite, beside, across, t)):
            value = dot(act[n], wd[j])
            sib_out[n, j] = value[seqs:].astype(bf16)
            mine[n, j] = value[:seqs]
            if number == 0 and n in early_out:
                remote(sib_out.at[n, j], sib_in.at[n, j], twin, "back", ("corner back", n))
        if n in early_out:
            for j in (beside, across, t):
                remote(sib_out.at[n, j], sib_in.at[n, j], twin, "back", ("back", n))
        else:
            remote(sib_out.at[n], sib_in.at[n], twin, "back", ("back", n))

    def add_twin(n, j):
        both = mine[n, j] + sib_in[n, j].astype(f32)
        mine[n, j] = both
        summed[n, j] = both.astype(bf16)

    def reduce_chip(n):
        if n in early_out:
            absorb(sib_in.at[n, 0], arrival(("corner back", n)))
            add_twin(n, opposite)
            if n not in direct_out:
                remote(summed.at[n, opposite, top], fwd_in.at[n, 0], side_b, "sum", ("fwd", n))
                remote(summed.at[n, opposite, bottom], fwd_in.at[n, 1], side_a, "sum", ("fwd", n))
            else:
                remote(summed.at[n, opposite], from_side.at[n, 2], side_o, "sum", ("mine", n))
            absorb(sib_in.at[n, 0 : tp - 1], arrival(("back", n)))
            add_twin(n, beside)
            add_twin(n, across)
            if n in direct_out:
                remote(summed.at[n, beside], from_side.at[n, 0], side_b, "sum", ("mine", n))
                remote(summed.at[n, across], from_side.at[n, 1], side_a, "sum", ("mine", n))
            else:
                remote(summed.at[n, beside, top], from_side.at[n, 0, top], side_b, "sum", ("mine", n))
                remote(summed.at[n, across, bottom], from_side.at[n, 1, bottom], side_a, "sum", ("mine", n))
            return
        absorb(sib_in.at[n], arrival(("back", n)))
        for j in (opposite, beside, across):
            add_twin(n, j)
        if n in direct_out:
            remote(summed.at[n, opposite], from_side.at[n, 2], side_o, "sum", ("mine", n))
            remote(summed.at[n, beside], from_side.at[n, 0], side_b, "sum", ("mine", n))
            remote(summed.at[n, across], from_side.at[n, 1], side_a, "sum", ("mine", n))
            return
        remote(summed.at[n, opposite, top], fwd_in.at[n, 0], side_b, "sum", ("fwd", n))
        remote(summed.at[n, opposite, bottom], fwd_in.at[n, 1], side_a, "sum", ("fwd", n))
        remote(summed.at[n, beside, top], from_side.at[n, 0, top], side_b, "sum", ("mine", n))
        remote(summed.at[n, across, bottom], from_side.at[n, 1, bottom], side_a, "sum", ("mine", n))

    def reduce_relay(n):
        if n in direct_out:
            return
        absorb(fwd_in.at[n], arrival(("fwd", n)))
        fwd_out[n, 0] = (mine[n, across, 0:half] + fwd_in[n, 0].astype(f32)).astype(bf16)
        fwd_out[n, 1] = (mine[n, beside, half:] + fwd_in[n, 1].astype(f32)).astype(bf16)
        remote(fwd_out.at[n, 0], from_side.at[n, 1, top], side_a, "sum", ("mine", n))
        remote(fwd_out.at[n, 1], from_side.at[n, 0, bottom], side_b, "sum", ("mine", n))

    def go_home(n):
        value = mine[n, t] + sib_in[n, t].astype(f32)
        count = 3 if n in direct_out else 2
        absorb(from_side.at[n, 0:count], arrival(("mine", n)))
        for k in range(count):
            value = value + from_side[n, k].astype(f32)
        if n:
            home_out[n] = value.astype(bf16)
            remote(home_out.at[n], home_in.at[n], (flip(me, 2 * n), t), "home", "home")
        else:
            mine[n, t] = value

    def finish():
        result = stream_f + mine[0, t]
        absorb(home_in.at[0 : chips - 1], arrival("home"))
        for n in range(1, chips):
            result = result + home_in[n].astype(f32)
        out_ref[...] = result.astype(bf16)

    direct_in, direct_out = (), ()
    outs, early_out = (0, 1, 2, 3), (3,)
    plan = [
        (spread_chips,), (enter, 0), (logits,),
        (relay, 0), (enter, 1), (enter, 2), (weights,), (scale_in, 0, "t"), (corner, 0), (scale_in, 0, "ba"), (scale_in, 1, "t"), (relay, 1), (enter, 3),
        (scale_in, 0, "o"), (expert_in, 0), (relay, 2), (activate, 0), (scale_in, 1, "ba"), (corner, 1), (expert_out, 0), (relay, 3), (scale_in, 2, "t"), (scale_in, 2, "ba"), (scale_in, 1, "o"),
        (expert_in, 1), (corner, 2), (reduce_chip, 0), (activate, 1), (expert_out, 1), (scale_in, 3, "t"), (corner, 3), (scale_in, 3, "ba"),
        (scale_in, 2, "o"), (expert_in, 2), (reduce_chip, 1), (activate, 2), (expert_out, 2), (reduce_relay, 0),
        (scale_in, 3, "o"), (expert_in, 3), (reduce_chip, 2), (activate, 3), (expert_out, 3), (reduce_relay, 1), (go_home, 0),
        (reduce_chip, 3), (reduce_relay, 2), (go_home, 1), (reduce_relay, 3), (go_home, 2), (go_home, 3),
        (finish,),
    ]
    for step in plan:
        step[0](*step[1:])
    spent = {
        "g0": res_all.at[0 : tp - 1],
        "g1": mix_all.at[0 : tp - 1],
        "g2": gated_all.at[0 : tp - 1],
        "g3": logit_all.at[0 : tp - 1],
        "weight": weight_all.at[0 : ep - 1],
        "chips": home_in.at[0 : chips - 1],
        "side": tok.at[0],
        "relay": tok.at[0, 0 : tp // 2],
        "twin": tok.at[0:2],
        "back": sib_in,
        "home": home_in.at[0 : chips - 1],
    }
    for kind, ref in spent.items():
        absorb(ref, send_sem.at[SENDS.index(kind)])
    absorb(sib_in.at[:, 0:3], send_sem.at[SENDS.index("sum")])


def finish_kernel(a_in, b_in, c_in, a_out, b_out, c_out, sems):
    writes = [
        pltpu.make_async_copy(held, target, sems.at[n])
        for n, (held, target) in enumerate(((a_in, a_out), (b_in, b_out), (c_in, c_out)))
    ]
    for write in writes:
        write.start()
    for write in writes:
        write.wait()


def dispatch(*args):
    (
        residual, state_re, state_im, mix_gain, proj_in, decay_rate, frequency, log_step,
        input_re, input_im, read_re, read_im, skip_gain, glu_weight, out_proj, ffn_gain,
        router, gate_weight, up_weight, down_weight, route_ids,
    ) = args
    ep, tp = lax.axis_size("ep"), lax.axis_size("tp")
    seqs, cols = residual.shape
    groups, states = decay_rate.shape
    chans = skip_gain.shape[0]
    rough = groups % 16 or chans % 128 or cols % 128 or seqs % 32 or seqs > 128
    if gate_weight.shape[0] != 1 or tp != 4 or ep != 8 or rough:
        return per_device(*args)
    top = route_ids.shape[1]
    hidden = gate_weight.shape[2]
    width = mix_gain.shape[0]
    chips = ep // 2
    bf16, f32 = jnp.bfloat16, jnp.float32
    hbm, vmem = pl.BlockSpec(memory_space=pltpu.HBM), pl.BlockSpec(memory_space=pltpu.VMEM)
    state_shape = (seqs, groups, states)
    blocks = (chips, tp, seqs, cols)
    out = pl.pallas_call(
        functools.partial(layer_kernel, (ep, tp)),
        out_shape=(
            pltpu.VMEM((seqs, cols), bf16),
            pltpu.VMEM(state_shape, f32),
            pltpu.VMEM(state_shape, f32),
        ),
        in_specs=[hbm] * 21,
        out_specs=(vmem, vmem, vmem),
        scratch_shapes=[
            pltpu.VMEM((seqs, cols), bf16),
            pltpu.VMEM((2, tp, 1, cols), f32),
            pltpu.VMEM((2, groups, states), f32),
            pltpu.VMEM((1, groups), f32),
            pltpu.VMEM((2, groups, chans // groups, states), f32),
            pltpu.VMEM((2, chans, states), f32),
            pltpu.VMEM((1, chans), f32),
            pltpu.VMEM((ep, width), f32),
            pltpu.VMEM((top, seqs), jnp.int32),
            pltpu.VMEM((2,) + state_shape, f32),
            pltpu.VMEM(proj_in.shape, bf16),
            pltpu.VMEM(glu_weight.shape, bf16),
            pltpu.VMEM(out_proj.shape, bf16),
            pltpu.VMEM((width, 2 * hidden), bf16),
            pltpu.VMEM((tp, hidden, cols), bf16),
            pltpu.VMEM((tp, seqs, cols), bf16),
            pltpu.VMEM((tp, seqs, chans), bf16),
            pltpu.VMEM((tp, seqs, chans), bf16),
            pltpu.VMEM((tp, 2 * ep, 128), f32),
            pltpu.VMEM((ep, 2 * ep, 128), f32),
            pltpu.VMEM((chips, tp, 2 * seqs, cols), bf16),
            pltpu.VMEM((chips, 2 * seqs, width), bf16),
            pltpu.VMEM((2 * seqs, 2 * hidden), f32),
            pltpu.VMEM((chips, 2 * seqs, hidden), bf16),
            pltpu.VMEM(blocks, f32),
            pltpu.VMEM(blocks, bf16),
            pltpu.VMEM(blocks, bf16),
            pltpu.VMEM(blocks, bf16),
            pltpu.VMEM((chips, 3, seqs, cols), bf16),
            pltpu.VMEM((chips, 2, seqs // 2, cols), bf16),
            pltpu.VMEM((chips, 2, seqs // 2, cols), bf16),
            pltpu.VMEM((chips, seqs, cols), bf16),
            pltpu.VMEM((chips, seqs, cols), bf16),
            pltpu.SemaphoreType.DMA((15,)),
            pltpu.SemaphoreType.DMA((len(SENDS),)),
            pltpu.SemaphoreType.DMA((42,)),
        ],
        compiler_params=pltpu.CompilerParams(
            collective_id=0, has_side_effects=True, vmem_limit_bytes=48 * 1024 * 1024
        ),
        name="layer",
    )(*(pltpu.with_memory_space_constraint(part, pltpu.HBM) for part in (
        residual,
        mix_gain.reshape(tp, 1, cols),
        ffn_gain.reshape(tp, 1, cols),
        decay_rate,
        frequency,
        log_step.reshape(1, groups),
        input_re.transpose(0, 2, 1),
        input_im.transpose(0, 2, 1),
        read_re.reshape(chans, states),
        read_im.reshape(chans, states),
        skip_gain.reshape(1, chans),
        router.T,
        route_ids.T,
        state_re,
        state_im,
        proj_in,
        glu_weight,
        out_proj,
        gate_weight.reshape(gate_weight.shape[1:]),
        up_weight.reshape(up_weight.shape[1:]),
        down_weight.reshape(down_weight.shape[1:]),
    )))
    return pl.pallas_call(
        finish_kernel,
        out_shape=tuple(jax.ShapeDtypeStruct(part.shape, part.dtype) for part in out),
        in_specs=[vmem] * 3,
        out_specs=(hbm,) * 3,
        scratch_shapes=[pltpu.SemaphoreType.DMA((3,))],
        compiler_params=pltpu.CompilerParams(vmem_limit_bytes=8 * 1024 * 1024),
        name="finish",
    )(*out)


def solution(mesh):
    in_specs = (
        P("ep", "tp"),
        P("ep", "tp", None),
        P("ep", "tp", None),
        P(),
        P(None, "tp"),
        P("tp", None),
        P("tp", None),
        P("tp"),
        P("tp", None, None),
        P("tp", None, None),
        P("tp", None, None),
        P("tp", None, None),
        P("tp"),
        P(None, "tp"),
        P(None, "tp"),
        P(),
        P(),
        P("ep", None, "tp"),
        P("ep", None, "tp"),
        P("ep", "tp", None),
        P("ep", None),
    )
    out_specs = (P("ep", "tp"), P("ep", "tp", None), P("ep", "tp", None))
    return jax.shard_map(
        dispatch, mesh=mesh, in_specs=in_specs, out_specs=out_specs, check_vma=False
    )
```

```python
import functools

import jax
import jax.numpy as jnp
from jax import lax
from jax.experimental import pallas as pl
from jax.experimental.pallas import tpu as pltpu
from jax.sharding import PartitionSpec as P

EPSILON = 1e-05
LIMIT = 7.0
ALPHA = 1.702


def discretise(decay_rate, frequency, log_step, input_re, input_im):
    real_part = -decay_rate
    step_size = jnp.exp(log_step)[:, None]
    magnitude = jnp.exp(step_size * real_part)
    abar_re = magnitude * jnp.cos(step_size * frequency)
    abar_im = magnitude * jnp.sin(step_size * frequency)
    denom = real_part * real_part + frequency * frequency
    minus_one = abar_re - 1.0
    coef_re = (minus_one * real_part + abar_im * frequency) / denom
    coef_im = (abar_im * real_part - minus_one * frequency) / denom
    bbar_re = coef_re[..., None] * input_re - coef_im[..., None] * input_im
    bbar_im = coef_re[..., None] * input_im + coef_im[..., None] * input_re
    return (abar_re, abar_im, bbar_re, bbar_im)


def per_device(
    residual,
    state_re,
    state_im,
    mix_gain,
    proj_in,
    decay_rate,
    frequency,
    log_step,
    input_re,
    input_im,
    read_re,
    read_im,
    skip_gain,
    glu_weight,
    out_proj,
    ffn_gain,
    router,
    gate_weight,
    up_weight,
    down_weight,
    route_ids,
):
    high = lax.Precision.HIGHEST
    seq_rows = residual.shape[0]
    col_count = residual.shape[1]
    width = mix_gain.shape[0]
    ep_size = lax.axis_size("ep")
    own_resid = residual.astype(jnp.float32)
    full_resid = lax.all_gather(residual, "tp", axis=1, tiled=True).astype(jnp.float32)
    scale_one = lax.rsqrt(jnp.mean(full_resid * full_resid, axis=1, keepdims=True) + EPSILON)
    xnorm = (full_resid * scale_one * mix_gain).astype(jnp.bfloat16)
    mix_in = jnp.dot(xnorm, proj_in, preferred_element_type=jnp.float32).astype(jnp.bfloat16)
    mix_f = mix_in.astype(jnp.float32)
    group_count = decay_rate.shape[0]
    group_width = input_re.shape[2]
    grouped = mix_f.reshape(seq_rows, group_count, group_width)
    abar_re, abar_im, bbar_re, bbar_im = discretise(
        decay_rate, frequency, log_step, input_re, input_im
    )
    drive_re = jnp.einsum("sgc,gnc->sgn", grouped, bbar_re, precision=high)
    drive_im = jnp.einsum("sgc,gnc->sgn", grouped, bbar_im, precision=high)
    state_re_new = abar_re * state_re - abar_im * state_im + drive_re
    state_im_new = abar_re * state_im + abar_im * state_re + drive_im
    readout = jnp.einsum("sgn,gcn->sgc", state_re_new, read_re, precision=high) - jnp.einsum(
        "sgn,gcn->sgc", state_im_new, read_im, precision=high
    )
    mixer = jax.nn.gelu(
        readout.reshape(seq_rows, group_count * group_width) + skip_gain * mix_f, approximate=False
    )
    all_mixer = lax.all_gather(mixer.astype(jnp.bfloat16), "tp", axis=1, tiled=True)
    glu_gate = jnp.dot(all_mixer, glu_weight, preferred_element_type=jnp.float32)
    gated = (mixer * jax.nn.sigmoid(glu_gate)).astype(jnp.bfloat16)
    all_gated = lax.all_gather(gated, "tp", axis=1, tiled=True)
    mixed = jnp.dot(all_gated, out_proj, preferred_element_type=jnp.float32)
    stream = (own_resid + mixed).astype(jnp.bfloat16)
    stream_f = stream.astype(jnp.float32)
    all_stream = lax.all_gather(stream, "tp", axis=1, tiled=True).astype(jnp.float32)
    inverse = lax.rsqrt(jnp.mean(all_stream * all_stream, axis=1, keepdims=True) + EPSILON)
    logits = jnp.dot(all_stream * ffn_gain, router, precision=high) * inverse
    payload = (all_stream * inverse * ffn_gain).astype(jnp.bfloat16)
    expert_count = router.shape[1]
    top_count = route_ids.shape[1]
    capacity = seq_rows * top_count // expert_count + 1
    expert_iota = jnp.arange(expert_count, dtype=jnp.int32)
    choose = (route_ids[:, :, None] == expert_iota).astype(jnp.float32)
    picked = jnp.sum(choose * logits[:, None, :], axis=2)
    expon = jnp.exp(picked)
    weights = expon / jnp.sum(expon, axis=1, keepdims=True)
    flat_route = route_ids.reshape(seq_rows * top_count)
    one_hot = (flat_route[:, None] == expert_iota).astype(jnp.int32)
    before = jnp.cumsum(one_hot, axis=0) - one_hot
    slot_ids = jnp.sum(before * one_hot, axis=1)
    target = flat_route * capacity + slot_ids
    slot_iota = jnp.arange(expert_count * capacity, dtype=jnp.int32)
    placing = jnp.any(slot_iota[:, None, None] == target.reshape(seq_rows, top_count)[None], axis=2)
    buffer = jnp.dot(placing.astype(jnp.bfloat16), payload, preferred_element_type=jnp.float32)
    buffer = buffer.astype(jnp.bfloat16).reshape(expert_count, capacity, payload.shape[1])
    local_experts = gate_weight.shape[0]
    received = lax.all_to_all(buffer, "ep", split_axis=0, concat_axis=0, tiled=True)
    items = received.shape[1]
    tokens = received.reshape(ep_size, local_experts, items, width)
    tokens = tokens.transpose(1, 0, 2, 3).reshape(local_experts, ep_size * items, width)
    gate_pre = jnp.einsum("esd,edf->esf", tokens, gate_weight, preferred_element_type=jnp.float32)
    up_pre = jnp.einsum("esd,edf->esf", tokens, up_weight, preferred_element_type=jnp.float32)
    gate_cl = jnp.minimum(gate_pre, LIMIT)
    up_cl = jnp.clip(up_pre, -LIMIT, LIMIT)
    active = ((up_cl + 1.0) * (gate_cl * jax.nn.sigmoid(ALPHA * gate_cl))).astype(jnp.bfloat16)
    partial_value = jnp.einsum(
        "esf,efd->esd", active, down_weight, preferred_element_type=jnp.float32
    ).astype(jnp.bfloat16)
    summed = lax.psum_scatter(
        partial_value.astype(jnp.float32).astype(jnp.bfloat16),
        "tp",
        scatter_dimension=2,
        tiled=True,
    )
    outgoing = summed.reshape(local_experts, ep_size, items, col_count)
    outgoing = outgoing.transpose(1, 0, 2, 3).reshape(ep_size * local_experts, items, col_count)
    returned = lax.all_to_all(outgoing, "ep", split_axis=0, concat_axis=0, tiled=True)
    flat_back = returned.reshape(expert_count * capacity, col_count)
    fetched = (
        jnp.take(flat_back, target, axis=0)
        .astype(jnp.float32)
        .reshape(seq_rows, top_count, col_count)
    )
    experts_sum = jnp.sum(weights[..., None] * fetched, axis=1)
    layer_out = (stream_f + experts_sum).astype(jnp.bfloat16)
    return (layer_out, state_re_new, state_im_new)


def erf(x):
    x = jnp.clip(x, -3.832506856900711, 3.832506856900711)
    y = x * x
    top = 0.00022905065861350646
    for coefficient in (
        0.0034082910107109506,
        0.050955695062380861,
        0.18520832239976145,
        1.128379143519084,
    ):
        top = top * y + coefficient
    bottom = -1.1791602954361697e-7
    for coefficient in (
        0.000023547966471313185,
        0.0010179625278914885,
        0.014070470171167667,
        0.11098505178285362,
        0.49746925110067538,
        1.0,
    ):
        bottom = bottom * y + coefficient
    return x * top / bottom


SENDS = ("rows", "g3", "weight")


def layer_kernel(
    sizes,
    resid_hbm,
    gain1_hbm,
    gain2_hbm,
    decay_hbm,
    freq_hbm,
    step_hbm,
    in_re_hbm,
    in_im_hbm,
    read_re_hbm,
    read_im_hbm,
    skip_hbm,
    router_hbm,
    route_hbm,
    sre_hbm,
    sim_hbm,
    proj_hbm,
    glu_hbm,
    outp_hbm,
    gate_hbm,
    up_hbm,
    down_hbm,
    out_ref,
    sre_out,
    sim_out,
    resid_ref,
    gains,
    poles,
    step_ref,
    in_maps,
    read_maps,
    skip_ref,
    router_ref,
    route_ref,
    state,
    proj,
    glu,
    outp,
    wgu,
    wd,
    res_all,
    mix_all,
    gated_all,
    logit_all,
    weight_all,
    tok,
    ready,
    acc,
    act,
    mine,
    sib_out,
    sib_in,
    summed,
    from_side,
    fwd_in,
    fwd_out,
    home_out,
    home_in,
    load_sem,
    send_sem,
    recv_sem,
):
    ep, tp = sizes
    rows = 2 * resid_ref.shape[0]
    f32, bf16 = jnp.float32, jnp.bfloat16
    me, t = lax.axis_index("ep"), lax.axis_index("tp")
    seqs, cols = resid_ref.shape
    width = cols * tp
    _, groups, states = poles.shape
    chans = skip_ref.shape[1]
    group_width = chans // groups
    chips = ep // 2
    half = seqs // 2
    hidden = wd.shape[1]
    last = (((1,), (1,)), ((), ()))

    def dot(a, b):
        return jnp.dot(a, b, preferred_element_type=f32)

    batches = {
        "resid": (resid_ref, [(resid_hbm, resid_ref)]),
        "route": (route_ref, [(route_hbm, route_ref)]),
        "step": (step_ref, [(step_hbm, step_ref)]),
        "poles": (poles, [(decay_hbm, poles.at[0]), (freq_hbm, poles.at[1])]),
        "in": (in_maps, [(in_re_hbm, in_maps.at[0]), (in_im_hbm, in_maps.at[1])]),
        "gains": (gains, [(gain1_hbm, gains.at[0]), (gain2_hbm, gains.at[1])]),
        "proj": (proj, [(proj_hbm, proj)]),
        "state": (state, [(sre_hbm, state.at[0]), (sim_hbm, state.at[1])]),
        "read": (read_maps, [(read_re_hbm, read_maps.at[0]), (read_im_hbm, read_maps.at[1])]),
        "skip": (skip_ref, [(skip_hbm, skip_ref)]),
        "glu": (glu, [(glu_hbm, glu)]),
        "outp": (outp, [(outp_hbm, outp)]),
        "router": (router_ref, [(router_hbm, router_ref)]),
        "experts": (wgu, [(gate_hbm, wgu.at[:, 0:hidden]), (up_hbm, wgu.at[:, hidden : 2 * hidden])]),
        "down": (wd, [(down_hbm.at[:, j * cols : (j + 1) * cols], wd.at[j]) for j in range(tp)]),
    }
    names = list(batches)

    def absorb(ref, sem):
        pltpu.make_async_copy(ref, ref, sem).wait()

    def loaded(*wanted):
        for name in wanted:
            absorb(batches[name][0], load_sem.at[names.index(name)])

    for n, name in enumerate(names):
        for source, held in batches[name][1]:
            pltpu.make_async_copy(source, held, load_sem.at[n]).start()

    barrier = pltpu.get_barrier_semaphore()
    for k in range(1, tp):
        pl.semaphore_signal(barrier, inc=1, device_id=(me, (t + k) % tp), device_id_type=pl.DeviceIdType.MESH)
    for k in range(1, ep):
        pl.semaphore_signal(barrier, inc=1, device_id=((me + k) % ep, t), device_id_type=pl.DeviceIdType.MESH)
    pl.semaphore_wait(barrier, tp + ep - 2)

    arrivals = []

    def arrival(key):
        if key[0] == "fwd":
            key = ("side", key[1], 0)
        elif key[0] == "corner back":
            key = ("side", key[1], 1)
        elif key[0] == "back":
            key = ("corner", key[1])
        elif key[0] == "mine":
            key = ("g%d" % (key[1] // 2), key[1] % 2)
        elif key == "home":
            key = ("g2", 0)
        if key not in arrivals:
            arrivals.append(key)
        return recv_sem.at[arrivals.index(key)]

    def remote(source, target, peer, kind, key):
        pltpu.make_async_remote_copy(
            src_ref=source,
            dst_ref=target,
            send_sem=send_sem.at[SENDS.index(kind if kind in SENDS else SENDS[0])],
            recv_sem=arrival(key),
            device_id=peer,
            device_id_type=pl.DeviceIdType.MESH,
        ).start()

    def flip(value, k):
        for bit in (1, 2, 4, 8, 16):
            if k & bit:
                value = value + bit - 2 * bit * ((value // bit) % 2)
        return value

    beside, across = flip(t, 1), flip(t, 2)
    opposite = flip(beside, 2)
    sibling = flip(me, 1)
    side_b, side_a, side_o, twin = (me, beside), (me, across), (me, opposite), (sibling, t)

    def gather(source, target, kind, key):
        for k in (3, 1, 2):
            remote(source, target, (me, flip(t, k)), kind, key)

    halves = [pl.ds(h * half, half) for h in range(2)]

    loaded("resid")
    for h in range(2):
        gather(resid_ref.at[halves[h]], res_all.at[t, halves[h]], "g0", ("g0", h))
    res_all[t] = resid_ref[...]

    loaded("route", "step", "poles", "in")
    square = (groups, groups)
    diagonal = lax.broadcasted_iota(jnp.int32, square, 0) == lax.broadcasted_iota(jnp.int32, square, 1)
    log_step = jnp.sum(
        jnp.where(diagonal, jnp.broadcast_to(step_ref[...], square), 0.0), axis=1, keepdims=True
    )
    step_size = jnp.exp(log_step)
    real_part, imag_part = -poles[0], poles[1]
    magnitude = jnp.exp(step_size * real_part)
    abar_re = magnitude * jnp.cos(step_size * imag_part)
    abar_im = magnitude * jnp.sin(step_size * imag_part)
    denom = real_part * real_part + imag_part * imag_part
    minus_one = abar_re - 1.0
    coef_re = ((minus_one * real_part + abar_im * imag_part) / denom)[:, None, :]
    coef_im = ((abar_im * real_part - minus_one * imag_part) / denom)[:, None, :]
    in_re, in_im = in_maps[0], in_maps[1]
    bb_re = (coef_re * in_re - coef_im * in_im).astype(bf16).reshape(chans, states)
    bb_im = (coef_re * in_im + coef_im * in_re).astype(bf16).reshape(chans, states)
    abar_re, abar_im = abar_re[None], abar_im[None]

    route = route_ref[...]
    iota_e = lax.broadcasted_iota(jnp.int32, (ep, seqs), 0)
    routed_t = jnp.zeros((ep, seqs), f32)
    for j in range(route.shape[0]):
        routed_t = routed_t + jnp.where(route[j : j + 1, :] == iota_e, 1.0, 0.0)
    row_i = lax.broadcasted_iota(jnp.int32, (seqs, seqs), 0)
    col_i = lax.broadcasted_iota(jnp.int32, (seqs, seqs), 1)

    held = {}
    flat = (half * groups, states)
    read_re, read_im = [], []

    def begin(h):
        if h == 0:
            loaded("gains", "proj")
        absorb(res_all.at[0 : tp - 1, 0:half], arrival(("g0", h)))
        total = jnp.zeros((half, 1), f32)
        for j in range(tp):
            part = res_all[j, halves[h]].astype(f32)
            total = total + jnp.sum(part * part, axis=1, keepdims=True)
        scale = lax.rsqrt(total / width + EPSILON)
        xnorm = [(res_all[j, halves[h]].astype(f32) * scale * gains[0, j]).astype(bf16) for j in range(tp)]
        mix = dot(jnp.concatenate(xnorm, axis=1), proj[...])
        mix_f = mix.astype(bf16).astype(f32)
        lane_c = lax.broadcasted_iota(jnp.int32, (half, groups, chans), 2)
        group_c = lax.broadcasted_iota(jnp.int32, (half, groups, chans), 1)
        first = group_c * group_width
        own = (lane_c >= first) & (lane_c < first + group_width)
        spread = jnp.where(own, jnp.broadcast_to(mix_f[:, None, :], own.shape), 0.0)
        spread = spread.astype(bf16).reshape(half * groups, chans)
        drive_re = dot(spread, bb_re).reshape(half, groups, states)
        drive_im = dot(spread, bb_im).reshape(half, groups, states)
        if h == 0:
            loaded("state", "read", "skip")
            read_re.append(read_maps[0].astype(bf16))
            read_im.append(read_maps[1].astype(bf16))
        old_re, old_im = state[0, halves[h]], state[1, halves[h]]
        new_re = abar_re * old_re - abar_im * old_im + drive_re
        new_im = abar_re * old_im + abar_im * old_re + drive_im
        sre_out[halves[h]] = new_re
        sim_out[halves[h]] = new_im
        readout = lax.dot_general(
            new_re.reshape(flat).astype(bf16), read_re[0], last, preferred_element_type=f32
        ) - lax.dot_general(
            new_im.reshape(flat).astype(bf16), read_im[0], last, preferred_element_type=f32
        )
        readout = jnp.sum(jnp.where(own, readout.reshape(half, groups, chans), 0.0), axis=1)
        pre = readout + skip_ref[...] * mix_f
        mixer = 0.5 * pre * (1.0 + erf(pre * 0.7071067811865476))
        held["mixer", h] = mixer
        mix_all[t, halves[h]] = mixer.astype(bf16)
        gather(mix_all.at[t, halves[h]], mix_all.at[t, halves[h]], "g1", ("g1", h))

    def gate(h):
        if h == 0:
            loaded("glu")
        absorb(mix_all.at[0 : tp - 1, 0:half], arrival(("g1", h)))
        glu_gate = dot(jnp.concatenate([mix_all[j, halves[h]] for j in range(tp)], axis=1), glu[...])
        gated_all[t, halves[h]] = (held["mixer", h] * jax.nn.sigmoid(glu_gate)).astype(bf16)
        gather(gated_all.at[t, halves[h]], gated_all.at[t, halves[h]], "g2", ("g2", h))

    def project(h):
        if h == 0:
            loaded("outp", "router")
        absorb(gated_all.at[0 : tp - 1, 0:half], arrival(("g2", h)))
        mixed = dot(jnp.concatenate([gated_all[j, halves[h]] for j in range(tp)], axis=1), outp[...])
        mixed = mixed + resid_ref[halves[h]].astype(f32)
        tok[0, t, halves[h]] = mixed.astype(bf16)
        for n in outs[1:]:
            remote(piece(0, t, h), piece(n, t, h), (flip(me, 2 * n), t), "chips", ("chips", n, h))
        enter(0, h)

    def piece(n, j, h, b=0):
        return tok.at[n, j, pl.ds(b * seqs + h * half, half)]

    def to_twin(n, key, j, h):
        remote(piece(n, j, h), piece(n, j, h, 1), twin, "twin", ("twin", n, key))

    def enter(n, h):
        if n:
            absorb(home_in.at[0, 0:half], arrival(("chips", n, h)))
        block = piece(n, t, h)
        if n in direct_in:
            remote(block, block, side_o, "relay", ("corner", n))
        remote(block, block, side_b, "side", ("side", n, h))
        remote(block, block, side_a, "side", ("side", n, h))
        to_twin(n, "tba", t, h)

    def relay(n, h):
        absorb(home_in.at[0:2, 0:half], arrival(("side", n, h)))
        if n not in direct_in:
            block, peer = (piece(n, beside, 0), side_a) if h == 0 else (piece(n, across, 1), side_b)
            remote(block, block, peer, "relay", ("corner", n))
        to_twin(n, "tba", beside, h)
        to_twin(n, "tba", across, h)

    def corner(n):
        absorb(home_in.at[0], arrival(("corner", n)))
        whole = tok.at[n, opposite, pl.ds(0, seqs)]
        remote(whole, tok.at[n, opposite, pl.ds(seqs, seqs)], twin, "twin", ("twin", n, "o"))

    def logits():
        stream_f = tok[0, t, 0:seqs].astype(f32)
        logit_all[t] = jnp.zeros(logit_all.shape[1:], f32)
        logit_all[t, 0:ep, 0:seqs] = lax.dot_general(
            router_ref[:, pl.ds(pl.multiple_of(t * cols, cols), cols)],
            stream_f * gains[1, t],
            last,
            precision=lax.Precision.HIGHEST,
            preferred_element_type=f32,
        )
        energy = jnp.sum(stream_f * stream_f, axis=1, keepdims=True)
        logit_all[t, ep : ep + 1, 0:seqs] = jnp.sum(
            jnp.where(row_i == col_i, energy, 0.0), axis=0, keepdims=True
        )
        gather(logit_all.at[t], logit_all.at[t], "g3", "g3")

    def weights():
        absorb(logit_all.at[0 : tp - 1], arrival("g3"))
        whole = logit_all[0]
        for j in range(1, tp):
            whole = whole + logit_all[j]
        whole = whole[:, 0:seqs]
        inverse = lax.rsqrt(whole[ep : ep + 1] / width + EPSILON)
        chosen = routed_t > 0.5
        expon = jnp.where(chosen, jnp.exp(jnp.where(chosen, whole[0:ep] * inverse, 0.0)), 0.0)
        weight_all[0] = jnp.zeros(weight_all.shape[1:], f32)
        weight_all[0, 0:ep, 0:seqs] = expon / jnp.sum(expon, axis=0, keepdims=True)
        weight_all[0, ep : ep + 1, 0:seqs] = inverse
        for k in range(1, ep):
            remote(weight_all.at[0], weight_all.at[k], (flip(me, k), t), "weight", "weight")

    def scale_in(n, key):
        places = {"tba": [t, beside, across], "o": [opposite]}[key]
        absorb(res_all.at[0 : len(places)], arrival(("twin", n, key)))
        for j in places:
            span = pl.ds(pl.multiple_of(j * cols, cols), cols)
            ready[n, :, span] = (tok[n, j].astype(f32) * gains[1, j]).astype(bf16)

    def expert_in(n):
        if n == outs[0]:
            loaded("experts")
        acc[...] = dot(ready[n], wgu[...])

    def expert_gate(n):
        if n == outs[0]:
            loaded("experts")
        acc[:, 0:hidden] = dot(ready[n], wgu[:, 0:hidden])

    def expert_up(n):
        acc[:, hidden:] = dot(ready[n], wgu[:, hidden:])

    def column(line):
        return jnp.sum(jnp.where(row_i == col_i, line, 0.0), axis=1, keepdims=True)

    def activate(n):
        if n == outs[0]:
            absorb(weight_all.at[0 : ep - 1], arrival("weight"))
        for b in range(2):
            lines = slice(b * seqs, (b + 1) * seqs)
            norm = column(weight_all[2 * n + b, ep : ep + 1, 0:seqs])
            share = column(weight_all[2 * n + b, pl.ds(me, 1), 0:seqs])
            gate_cl = jnp.minimum(acc[lines, 0:hidden] * norm, LIMIT)
            up_cl = jnp.clip(acc[lines, hidden:] * norm, -LIMIT, LIMIT)
            act[n, lines] = (((up_cl + 1.0) * share) * (gate_cl * jax.nn.sigmoid(ALPHA * gate_cl))).astype(bf16)

    def expert_out(n):
        if n == outs[0]:
            loaded("down")
        for number, j in enumerate((opposite, beside, across, t)):
            value = dot(act[n], wd[j])
            sib_out[n, j] = value[seqs:].astype(bf16)
            mine[n, j] = value[:seqs]
            if number == 0 and n in early_out:
                remote(sib_out.at[n, j], sib_in.at[n, j], twin, "back", ("corner back", n))
        if n in early_out:
            for j in (beside, across, t):
                remote(sib_out.at[n, j], sib_in.at[n, j], twin, "back", ("back", n))
        else:
            remote(sib_out.at[n], sib_in.at[n], twin, "back", ("back", n))

    def add_twin(n, j):
        both = mine[n, j] + sib_in[n, j].astype(f32)
        mine[n, j] = both
        summed[n, j] = both.astype(bf16)

    def cut(n, p, side=0):
        size = half // (2 if n in split_out else 1)
        return pl.ds(side * half + p * size, size)

    def parts(n):
        return range(2 if n in split_out else 1)

    def reduce_corner(n):
        if n in early_out:
            absorb(sib_in.at[n, 0], arrival(("corner back", n)))
        else:
            absorb(sib_in.at[n], arrival(("back", n)))
        add_twin(n, opposite)
        for p in parts(n):
            for side, peer in ((0, side_b), (1, side_a)):
                block = summed.at[n, opposite, cut(n, p, side)]
                remote(block, fwd_in.at[n, side, cut(n, p)], peer, "sum", ("fwd", n, p))

    def reduce_sides(n):
        if n in early_out:
            absorb(sib_in.at[n, 0 : tp - 1], arrival(("back", n)))
        add_twin(n, beside)
        add_twin(n, across)
        for p in parts(n):
            for side, peer, j in ((0, side_b, beside), (1, side_a, across)):
                block = summed.at[n, j, cut(n, p, side)]
                remote(block, from_side.at[n, side, cut(n, p, side)], peer, "sum", ("mine", n, p))

    def reduce_chip(n):
        reduce_corner(n)
        reduce_sides(n)

    def reduce_relay(n, p=0):
        here = cut(n, p)
        absorb(fwd_in.at[n, :, here], arrival(("fwd", n, p)))
        for side, peer, j in ((0, side_a, across), (1, side_b, beside)):
            there = cut(n, p, side)
            fwd_out[n, side, here] = (mine[n, j, there] + fwd_in[n, side, here].astype(f32)).astype(bf16)
            remote(fwd_out.at[n, side, here], from_side.at[n, 1 - side, there], peer, "sum", ("mine", n, p))

    def go_home(n, p=0):
        size = half // len(parts(n))
        absorb(from_side.at[n, 0:2, 0 : 2 * size], arrival(("mine", n, p)))
        for side in range(2):
            there = cut(n, p, side)
            value = mine[n, t, there] + sib_in[n, t, there].astype(f32)
            value = value + from_side[n, 0, there].astype(f32) + from_side[n, 1, there].astype(f32)
            if n:
                home_out[n, there] = value.astype(bf16)
                remote(home_out.at[n, there], home_in.at[n, there], (flip(me, 2 * n), t), "home", "home")
            else:
                mine[n, t, there] = value

    def finish():
        result = tok[0, t, 0:seqs].astype(f32) + mine[0, t]
        absorb(home_in.at[0 : chips - 1], arrival("home"))
        for n in range(1, chips):
            result = result + home_in[n].astype(f32)
        out_ref[...] = result.astype(bf16)

    outs, early_out, split_out, direct_in = (0, 1, 2, 3), (3,), (), ()
    plan = [
        (begin, 0), (begin, 1), (gate, 0), (gate, 1), (project, 0), (project, 1), (logits,), (relay, 0, 0),
        (enter, 1, 0), (relay, 0, 1), (enter, 1, 1), (enter, 2, 0), (enter, 2, 1), (weights,), (relay, 1, 0),
        (corner, 0), (scale_in, 0, "tba"), (relay, 1, 1), (enter, 3, 0), (enter, 3, 1), (scale_in, 0, "o"),
        (expert_in, 0), (relay, 2, 0), (relay, 2, 1), (activate, 0), (scale_in, 1, "tba"), (corner, 1),
        (expert_out, 0), (relay, 3, 0), (relay, 3, 1), (scale_in, 2, "tba"), (scale_in, 1, "o"), (expert_in, 1),
        (corner, 2), (reduce_chip, 0), (activate, 1), (expert_out, 1), (corner, 3), (scale_in, 3, "tba"),
        (scale_in, 2, "o"), (expert_in, 2), (reduce_chip, 1), (activate, 2), (expert_out, 2), (reduce_relay, 0),
        (scale_in, 3, "o"), (expert_in, 3), (reduce_chip, 2), (activate, 3), (expert_out, 3), (reduce_relay, 1),
        (go_home, 0), (reduce_chip, 3), (reduce_relay, 2), (go_home, 1), (reduce_relay, 3), (go_home, 2),
        (go_home, 3), (finish,),
    ]
    for step in plan:
        step[0](*step[1:])
    block = seqs * cols
    sent = 3 * block + 6 * seqs * chans + (chips - 1) * 2 * block + chips * (2 + 1 + 4 + 4 + 3) * block
    absorb(wgu.at[0 : sent // (2 * hidden)], send_sem.at[SENDS.index("rows")])
    absorb(logit_all.at[0 : tp - 1], send_sem.at[SENDS.index("g3")])
    absorb(weight_all.at[0 : ep - 1], send_sem.at[SENDS.index("weight")])


def finish_kernel(a_in, b_in, c_in, a_out, b_out, c_out, sems):
    writes = [
        pltpu.make_async_copy(held, target, sems.at[n])
        for n, (held, target) in enumerate(((a_in, a_out), (b_in, b_out), (c_in, c_out)))
    ]
    for write in writes:
        write.start()
    for write in writes:
        write.wait()


def dispatch(*args):
    (
        residual, state_re, state_im, mix_gain, proj_in, decay_rate, frequency, log_step,
        input_re, input_im, read_re, read_im, skip_gain, glu_weight, out_proj, ffn_gain,
        router, gate_weight, up_weight, down_weight, route_ids,
    ) = args
    ep, tp = lax.axis_size("ep"), lax.axis_size("tp")
    seqs, cols = residual.shape
    groups, states = decay_rate.shape
    chans = skip_gain.shape[0]
    rough = groups % 16 or chans % 128 or cols % 128 or seqs % 32 or seqs > 128
    if gate_weight.shape[0] != 1 or tp != 4 or ep != 8 or rough:
        return per_device(*args)
    top = route_ids.shape[1]
    hidden = gate_weight.shape[2]
    width = mix_gain.shape[0]
    chips = ep // 2
    bf16, f32 = jnp.bfloat16, jnp.float32
    hbm, vmem = pl.BlockSpec(memory_space=pltpu.HBM), pl.BlockSpec(memory_space=pltpu.VMEM)
    state_shape = (seqs, groups, states)
    blocks = (chips, tp, seqs, cols)
    out = pl.pallas_call(
        functools.partial(layer_kernel, (ep, tp)),
        out_shape=(
            pltpu.VMEM((seqs, cols), bf16),
            pltpu.VMEM(state_shape, f32),
            pltpu.VMEM(state_shape, f32),
        ),
        in_specs=[hbm] * 21,
        out_specs=(vmem, vmem, vmem),
        scratch_shapes=[
            pltpu.VMEM((seqs, cols), bf16),
            pltpu.VMEM((2, tp, 1, cols), f32),
            pltpu.VMEM((2, groups, states), f32),
            pltpu.VMEM((1, groups), f32),
            pltpu.VMEM((2, groups, chans // groups, states), f32),
            pltpu.VMEM((2, chans, states), f32),
            pltpu.VMEM((1, chans), f32),
            pltpu.VMEM((ep, width), f32),
            pltpu.VMEM((top, seqs), jnp.int32),
            pltpu.VMEM((2,) + state_shape, f32),
            pltpu.VMEM(proj_in.shape, bf16),
            pltpu.VMEM(glu_weight.shape, bf16),
            pltpu.VMEM(out_proj.shape, bf16),
            pltpu.VMEM((width, 2 * hidden), bf16),
            pltpu.VMEM((tp, hidden, cols), bf16),
            pltpu.VMEM((tp, seqs, cols), bf16),
            pltpu.VMEM((tp, seqs, chans), bf16),
            pltpu.VMEM((tp, seqs, chans), bf16),
            pltpu.VMEM((tp, 2 * ep, 128), f32),
            pltpu.VMEM((ep, 2 * ep, 128), f32),
            pltpu.VMEM((chips, tp, 2 * seqs, cols), bf16),
            pltpu.VMEM((chips, 2 * seqs, width), bf16),
            pltpu.VMEM((2 * seqs, 2 * hidden), f32),
            pltpu.VMEM((chips, 2 * seqs, hidden), bf16),
            pltpu.VMEM(blocks, f32),
            pltpu.VMEM(blocks, bf16),
            pltpu.VMEM(blocks, bf16),
            pltpu.VMEM(blocks, bf16),
            pltpu.VMEM((chips, 3, seqs, cols), bf16),
            pltpu.VMEM((chips, 2, seqs // 2, cols), bf16),
            pltpu.VMEM((chips, 2, seqs // 2, cols), bf16),
            pltpu.VMEM((chips, seqs, cols), bf16),
            pltpu.VMEM((chips, seqs, cols), bf16),
            pltpu.SemaphoreType.DMA((15,)),
            pltpu.SemaphoreType.DMA((len(SENDS),)),
            pltpu.SemaphoreType.DMA((34,)),
        ],
        compiler_params=pltpu.CompilerParams(
            collective_id=0, has_side_effects=True, vmem_limit_bytes=48 * 1024 * 1024
        ),
        name="layer",
    )(*(pltpu.with_memory_space_constraint(part, pltpu.HBM) for part in (
        residual,
        mix_gain.reshape(tp, 1, cols),
        ffn_gain.reshape(tp, 1, cols),
        decay_rate,
        frequency,
        log_step.reshape(1, groups),
        input_re.transpose(0, 2, 1),
        input_im.transpose(0, 2, 1),
        read_re.reshape(chans, states),
        read_im.reshape(chans, states),
        skip_gain.reshape(1, chans),
        router.T,
        route_ids.T,
        state_re,
        state_im,
        proj_in,
        glu_weight,
        out_proj,
        gate_weight.reshape(gate_weight.shape[1:]),
        up_weight.reshape(up_weight.shape[1:]),
        down_weight.reshape(down_weight.shape[1:]),
    )))
    return pl.pallas_call(
        finish_kernel,
        out_shape=tuple(jax.ShapeDtypeStruct(part.shape, part.dtype) for part in out),
        in_specs=[vmem] * 3,
        out_specs=(hbm,) * 3,
        scratch_shapes=[pltpu.SemaphoreType.DMA((3,))],
        compiler_params=pltpu.CompilerParams(vmem_limit_bytes=8 * 1024 * 1024),
        name="finish",
    )(*out)


def solution(mesh):
    in_specs = (
        P("ep", "tp"),
        P("ep", "tp", None),
        P("ep", "tp", None),
        P(),
        P(None, "tp"),
        P("tp", None),
        P("tp", None),
        P("tp"),
        P("tp", None, None),
        P("tp", None, None),
        P("tp", None, None),
        P("tp", None, None),
        P("tp"),
        P(None, "tp"),
        P(None, "tp"),
        P(),
        P(),
        P("ep", None, "tp"),
        P("ep", None, "tp"),
        P("ep", "tp", None),
        P("ep", None),
    )
    out_specs = (P("ep", "tp"), P("ep", "tp", None), P("ep", "tp", None))
    return jax.shard_map(
        dispatch, mesh=mesh, in_specs=in_specs, out_specs=out_specs, check_vma=False
    )
```

```python
import functools

import jax
import jax.numpy as jnp
from jax import lax
from jax.experimental import pallas as pl
from jax.experimental.pallas import tpu as pltpu
from jax.sharding import PartitionSpec as P

EPSILON = 1e-05
LIMIT = 7.0
ALPHA = 1.702


def discretise(decay_rate, frequency, log_step, input_re, input_im):
    real_part = -decay_rate
    step_size = jnp.exp(log_step)[:, None]
    magnitude = jnp.exp(step_size * real_part)
    abar_re = magnitude * jnp.cos(step_size * frequency)
    abar_im = magnitude * jnp.sin(step_size * frequency)
    denom = real_part * real_part + frequency * frequency
    minus_one = abar_re - 1.0
    coef_re = (minus_one * real_part + abar_im * frequency) / denom
    coef_im = (abar_im * real_part - minus_one * frequency) / denom
    bbar_re = coef_re[..., None] * input_re - coef_im[..., None] * input_im
    bbar_im = coef_re[..., None] * input_im + coef_im[..., None] * input_re
    return (abar_re, abar_im, bbar_re, bbar_im)


def per_device(
    residual,
    state_re,
    state_im,
    mix_gain,
    proj_in,
    decay_rate,
    frequency,
    log_step,
    input_re,
    input_im,
    read_re,
    read_im,
    skip_gain,
    glu_weight,
    out_proj,
    ffn_gain,
    router,
    gate_weight,
    up_weight,
    down_weight,
    route_ids,
):
    high = lax.Precision.HIGHEST
    seq_rows = residual.shape[0]
    col_count = residual.shape[1]
    width = mix_gain.shape[0]
    ep_size = lax.axis_size("ep")
    own_resid = residual.astype(jnp.float32)
    full_resid = lax.all_gather(residual, "tp", axis=1, tiled=True).astype(jnp.float32)
    scale_one = lax.rsqrt(jnp.mean(full_resid * full_resid, axis=1, keepdims=True) + EPSILON)
    xnorm = (full_resid * scale_one * mix_gain).astype(jnp.bfloat16)
    mix_in = jnp.dot(xnorm, proj_in, preferred_element_type=jnp.float32).astype(jnp.bfloat16)
    mix_f = mix_in.astype(jnp.float32)
    group_count = decay_rate.shape[0]
    group_width = input_re.shape[2]
    grouped = mix_f.reshape(seq_rows, group_count, group_width)
    abar_re, abar_im, bbar_re, bbar_im = discretise(
        decay_rate, frequency, log_step, input_re, input_im
    )
    drive_re = jnp.einsum("sgc,gnc->sgn", grouped, bbar_re, precision=high)
    drive_im = jnp.einsum("sgc,gnc->sgn", grouped, bbar_im, precision=high)
    state_re_new = abar_re * state_re - abar_im * state_im + drive_re
    state_im_new = abar_re * state_im + abar_im * state_re + drive_im
    readout = jnp.einsum("sgn,gcn->sgc", state_re_new, read_re, precision=high) - jnp.einsum(
        "sgn,gcn->sgc", state_im_new, read_im, precision=high
    )
    mixer = jax.nn.gelu(
        readout.reshape(seq_rows, group_count * group_width) + skip_gain * mix_f, approximate=False
    )
    all_mixer = lax.all_gather(mixer.astype(jnp.bfloat16), "tp", axis=1, tiled=True)
    glu_gate = jnp.dot(all_mixer, glu_weight, preferred_element_type=jnp.float32)
    gated = (mixer * jax.nn.sigmoid(glu_gate)).astype(jnp.bfloat16)
    all_gated = lax.all_gather(gated, "tp", axis=1, tiled=True)
    mixed = jnp.dot(all_gated, out_proj, preferred_element_type=jnp.float32)
    stream = (own_resid + mixed).astype(jnp.bfloat16)
    stream_f = stream.astype(jnp.float32)
    all_stream = lax.all_gather(stream, "tp", axis=1, tiled=True).astype(jnp.float32)
    inverse = lax.rsqrt(jnp.mean(all_stream * all_stream, axis=1, keepdims=True) + EPSILON)
    logits = jnp.dot(all_stream * ffn_gain, router, precision=high) * inverse
    payload = (all_stream * inverse * ffn_gain).astype(jnp.bfloat16)
    expert_count = router.shape[1]
    top_count = route_ids.shape[1]
    capacity = seq_rows * top_count // expert_count + 1
    expert_iota = jnp.arange(expert_count, dtype=jnp.int32)
    choose = (route_ids[:, :, None] == expert_iota).astype(jnp.float32)
    picked = jnp.sum(choose * logits[:, None, :], axis=2)
    expon = jnp.exp(picked)
    weights = expon / jnp.sum(expon, axis=1, keepdims=True)
    flat_route = route_ids.reshape(seq_rows * top_count)
    one_hot = (flat_route[:, None] == expert_iota).astype(jnp.int32)
    before = jnp.cumsum(one_hot, axis=0) - one_hot
    slot_ids = jnp.sum(before * one_hot, axis=1)
    target = flat_route * capacity + slot_ids
    slot_iota = jnp.arange(expert_count * capacity, dtype=jnp.int32)
    placing = jnp.any(slot_iota[:, None, None] == target.reshape(seq_rows, top_count)[None], axis=2)
    buffer = jnp.dot(placing.astype(jnp.bfloat16), payload, preferred_element_type=jnp.float32)
    buffer = buffer.astype(jnp.bfloat16).reshape(expert_count, capacity, payload.shape[1])
    local_experts = gate_weight.shape[0]
    received = lax.all_to_all(buffer, "ep", split_axis=0, concat_axis=0, tiled=True)
    items = received.shape[1]
    tokens = received.reshape(ep_size, local_experts, items, width)
    tokens = tokens.transpose(1, 0, 2, 3).reshape(local_experts, ep_size * items, width)
    gate_pre = jnp.einsum("esd,edf->esf", tokens, gate_weight, preferred_element_type=jnp.float32)
    up_pre = jnp.einsum("esd,edf->esf", tokens, up_weight, preferred_element_type=jnp.float32)
    gate_cl = jnp.minimum(gate_pre, LIMIT)
    up_cl = jnp.clip(up_pre, -LIMIT, LIMIT)
    active = ((up_cl + 1.0) * (gate_cl * jax.nn.sigmoid(ALPHA * gate_cl))).astype(jnp.bfloat16)
    partial_value = jnp.einsum(
        "esf,efd->esd", active, down_weight, preferred_element_type=jnp.float32
    ).astype(jnp.bfloat16)
    summed = lax.psum_scatter(
        partial_value.astype(jnp.float32).astype(jnp.bfloat16),
        "tp",
        scatter_dimension=2,
        tiled=True,
    )
    outgoing = summed.reshape(local_experts, ep_size, items, col_count)
    outgoing = outgoing.transpose(1, 0, 2, 3).reshape(ep_size * local_experts, items, col_count)
    returned = lax.all_to_all(outgoing, "ep", split_axis=0, concat_axis=0, tiled=True)
    flat_back = returned.reshape(expert_count * capacity, col_count)
    fetched = (
        jnp.take(flat_back, target, axis=0)
        .astype(jnp.float32)
        .reshape(seq_rows, top_count, col_count)
    )
    experts_sum = jnp.sum(weights[..., None] * fetched, axis=1)
    layer_out = (stream_f + experts_sum).astype(jnp.bfloat16)
    return (layer_out, state_re_new, state_im_new)


def erf(x):
    x = jnp.clip(x, -3.832506856900711, 3.832506856900711)
    y = x * x
    top = 0.00022905065861350646
    for coefficient in (
        0.0034082910107109506,
        0.050955695062380861,
        0.18520832239976145,
        1.128379143519084,
    ):
        top = top * y + coefficient
    bottom = -1.1791602954361697e-7
    for coefficient in (
        0.000023547966471313185,
        0.0010179625278914885,
        0.014070470171167667,
        0.11098505178285362,
        0.49746925110067538,
        1.0,
    ):
        bottom = bottom * y + coefficient
    return x * top / bottom


SENDS = ("rows", "g3", "weight")


def layer_kernel(
    sizes,
    resid_hbm,
    gain1_hbm,
    gain2_hbm,
    decay_hbm,
    freq_hbm,
    step_hbm,
    in_re_hbm,
    in_im_hbm,
    read_re_hbm,
    read_im_hbm,
    skip_hbm,
    router_hbm,
    route_hbm,
    sre_hbm,
    sim_hbm,
    proj_hbm,
    glu_hbm,
    outp_hbm,
    gate_hbm,
    up_hbm,
    down_hbm,
    out_ref,
    sre_out,
    sim_out,
    resid_ref,
    gains,
    poles,
    step_ref,
    in_maps,
    read_maps,
    skip_ref,
    router_ref,
    route_ref,
    state,
    proj,
    glu,
    outp,
    wgu,
    wd,
    res_all,
    mix_all,
    gated_all,
    logit_all,
    weight_all,
    tok,
    ready,
    act,
    mine,
    sib_out,
    sib_in,
    summed,
    from_side,
    fwd_in,
    fwd_out,
    home_out,
    home_in,
    load_sem,
    send_sem,
    recv_sem,
):
    ep, tp = sizes
    f32, bf16 = jnp.float32, jnp.bfloat16
    me, t = lax.axis_index("ep"), lax.axis_index("tp")
    seqs, cols = resid_ref.shape
    width = cols * tp
    _, groups, states = poles.shape
    chans = skip_ref.shape[1]
    group_width = chans // groups
    chips = ep // 2
    half = seqs // 2
    hidden = wd.shape[1]
    piece_cols = 512
    last = (((1,), (1,)), ((), ()))

    def dot(a, b):
        return jnp.dot(a, b, preferred_element_type=f32)

    batches = {
        "resid": (resid_ref, [(resid_hbm, resid_ref)]),
        "route": (route_ref, [(route_hbm, route_ref)]),
        "step": (step_ref, [(step_hbm, step_ref)]),
        "poles": (poles, [(decay_hbm, poles.at[0]), (freq_hbm, poles.at[1])]),
        "in": (in_maps, [(in_re_hbm, in_maps.at[0]), (in_im_hbm, in_maps.at[1])]),
        "gains": (gains, [(gain1_hbm, gains.at[0]), (gain2_hbm, gains.at[1])]),
        "proj": (proj, [(proj_hbm, proj)]),
        "state": (state, [(sre_hbm, state.at[0]), (sim_hbm, state.at[1])]),
        "read": (read_maps, [(read_re_hbm, read_maps.at[0]), (read_im_hbm, read_maps.at[1])]),
        "skip": (skip_ref, [(skip_hbm, skip_ref)]),
        "glu": (glu, [(glu_hbm, glu)]),
        "outp": (outp, [(outp_hbm, outp)]),
        "router": (router_ref, [(router_hbm, router_ref)]),
        "experts": (wgu, [(gate_hbm, wgu.at[:, 0:hidden]), (up_hbm, wgu.at[:, hidden : 2 * hidden])]),
        "down": (wd, [(down_hbm.at[:, j * cols : (j + 1) * cols], wd.at[j]) for j in range(tp)]),
    }
    names = list(batches)

    def absorb(ref, sem):
        pltpu.make_async_copy(ref, ref, sem).wait()

    def loaded(*wanted):
        for name in wanted:
            absorb(batches[name][0], load_sem.at[names.index(name)])

    for n, name in enumerate(names):
        for source, held in batches[name][1]:
            pltpu.make_async_copy(source, held, load_sem.at[n]).start()

    barrier = pltpu.get_barrier_semaphore()
    for k in range(1, tp):
        pl.semaphore_signal(barrier, inc=1, device_id=(me, (t + k) % tp), device_id_type=pl.DeviceIdType.MESH)
    for k in range(1, ep):
        pl.semaphore_signal(barrier, inc=1, device_id=((me + k) % ep, t), device_id_type=pl.DeviceIdType.MESH)
    pl.semaphore_wait(barrier, tp + ep - 2)

    arrivals = []

    def arrival(key):
        if key[0] == "fwd":
            key = ("side", key[1], 0)
        elif key[0] == "corner back":
            key = ("side", key[1], 1)
        elif key[0] == "back":
            key = ("corner", key[1])
        elif key[0] == "mine":
            key = ("g%d" % (key[1] // 2), key[1] % 2)
        elif key == "home":
            key = ("g2", 0)
        if key not in arrivals:
            arrivals.append(key)
        return recv_sem.at[arrivals.index(key)]

    def remote(source, target, peer, kind, key):
        pltpu.make_async_remote_copy(
            src_ref=source,
            dst_ref=target,
            send_sem=send_sem.at[SENDS.index(kind if kind in SENDS else SENDS[0])],
            recv_sem=arrival(key),
            device_id=peer,
            device_id_type=pl.DeviceIdType.MESH,
        ).start()

    def flip(value, k):
        for bit in (1, 2, 4, 8, 16):
            if k & bit:
                value = value + bit - 2 * bit * ((value // bit) % 2)
        return value

    beside, across = flip(t, 1), flip(t, 2)
    opposite = flip(beside, 2)
    sibling = flip(me, 1)
    side_b, side_a, side_o, twin = (me, beside), (me, across), (me, opposite), (sibling, t)

    def gather(source, target, kind, key):
        for k in (3, 1, 2):
            remote(source, target, (me, flip(t, k)), kind, key)

    halves = [pl.ds(h * half, half) for h in range(2)]

    loaded("resid")
    for h in range(2):
        gather(resid_ref.at[halves[h]], res_all.at[t, halves[h]], "g0", ("g0", h))
    res_all[t] = resid_ref[...]

    loaded("route", "step", "poles", "in")
    square = (groups, groups)
    diagonal = lax.broadcasted_iota(jnp.int32, square, 0) == lax.broadcasted_iota(jnp.int32, square, 1)
    log_step = jnp.sum(
        jnp.where(diagonal, jnp.broadcast_to(step_ref[...], square), 0.0), axis=1, keepdims=True
    )
    step_size = jnp.exp(log_step)
    real_part, imag_part = -poles[0], poles[1]
    magnitude = jnp.exp(step_size * real_part)
    abar_re = magnitude * jnp.cos(step_size * imag_part)
    abar_im = magnitude * jnp.sin(step_size * imag_part)
    denom = real_part * real_part + imag_part * imag_part
    minus_one = abar_re - 1.0
    coef_re = ((minus_one * real_part + abar_im * imag_part) / denom)[:, None, :]
    coef_im = ((abar_im * real_part - minus_one * imag_part) / denom)[:, None, :]
    in_re, in_im = in_maps[0], in_maps[1]
    bb_re = (coef_re * in_re - coef_im * in_im).astype(bf16).reshape(chans, states)
    bb_im = (coef_re * in_im + coef_im * in_re).astype(bf16).reshape(chans, states)
    abar_re, abar_im = abar_re[None], abar_im[None]

    route = route_ref[...]
    iota_e = lax.broadcasted_iota(jnp.int32, (ep, seqs), 0)
    routed_t = jnp.zeros((ep, seqs), f32)
    for j in range(route.shape[0]):
        routed_t = routed_t + jnp.where(route[j : j + 1, :] == iota_e, 1.0, 0.0)
    row_i = lax.broadcasted_iota(jnp.int32, (seqs, seqs), 0)
    col_i = lax.broadcasted_iota(jnp.int32, (seqs, seqs), 1)

    held = {}
    flat = (half * groups, states)
    read_re, read_im = [], []

    def begin(h):
        if h == 0:
            loaded("gains", "proj")
        absorb(res_all.at[0 : tp - 1, 0:half], arrival(("g0", h)))
        total = jnp.zeros((half, 1), f32)
        for j in range(tp):
            part = res_all[j, halves[h]].astype(f32)
            total = total + jnp.sum(part * part, axis=1, keepdims=True)
        scale = lax.rsqrt(total / width + EPSILON)
        xnorm = [(res_all[j, halves[h]].astype(f32) * scale * gains[0, j]).astype(bf16) for j in range(tp)]
        mix = dot(jnp.concatenate(xnorm, axis=1), proj[...])
        mix_f = mix.astype(bf16).astype(f32)
        lane_c = lax.broadcasted_iota(jnp.int32, (half, groups, chans), 2)
        group_c = lax.broadcasted_iota(jnp.int32, (half, groups, chans), 1)
        first = group_c * group_width
        own = (lane_c >= first) & (lane_c < first + group_width)
        spread = jnp.where(own, jnp.broadcast_to(mix_f[:, None, :], own.shape), 0.0)
        spread = spread.astype(bf16).reshape(half * groups, chans)
        drive_re = dot(spread, bb_re).reshape(half, groups, states)
        drive_im = dot(spread, bb_im).reshape(half, groups, states)
        if h == 0:
            loaded("state", "read", "skip")
            read_re.append(read_maps[0].astype(bf16))
            read_im.append(read_maps[1].astype(bf16))
        old_re, old_im = state[0, halves[h]], state[1, halves[h]]
        new_re = abar_re * old_re - abar_im * old_im + drive_re
        new_im = abar_re * old_im + abar_im * old_re + drive_im
        sre_out[halves[h]] = new_re
        sim_out[halves[h]] = new_im
        readout = lax.dot_general(
            new_re.reshape(flat).astype(bf16), read_re[0], last, preferred_element_type=f32
        ) - lax.dot_general(
            new_im.reshape(flat).astype(bf16), read_im[0], last, preferred_element_type=f32
        )
        readout = jnp.sum(jnp.where(own, readout.reshape(half, groups, chans), 0.0), axis=1)
        pre = readout + skip_ref[...] * mix_f
        mixer = 0.5 * pre * (1.0 + erf(pre * 0.7071067811865476))
        held["mixer", h] = mixer
        mix_all[t, halves[h]] = mixer.astype(bf16)
        gather(mix_all.at[t, halves[h]], mix_all.at[t, halves[h]], "g1", ("g1", h))

    def gate(h):
        if h == 0:
            loaded("glu")
        absorb(mix_all.at[0 : tp - 1, 0:half], arrival(("g1", h)))
        glu_gate = dot(jnp.concatenate([mix_all[j, halves[h]] for j in range(tp)], axis=1), glu[...])
        gated_all[t, halves[h]] = (held["mixer", h] * jax.nn.sigmoid(glu_gate)).astype(bf16)
        gather(gated_all.at[t, halves[h]], gated_all.at[t, halves[h]], "g2", ("g2", h))

    def project(h):
        if h == 0:
            loaded("outp", "router")
        absorb(gated_all.at[0 : tp - 1, 0:half], arrival(("g2", h)))
        mixed = dot(jnp.concatenate([gated_all[j, halves[h]] for j in range(tp)], axis=1), outp[...])
        mixed = mixed + resid_ref[halves[h]].astype(f32)
        tok[0, t, halves[h]] = mixed.astype(bf16)
        for n in outs[1:]:
            remote(piece(0, t, h), piece(n, t, h), (flip(me, 2 * n), t), "chips", ("chips", n, h))
        enter(0, h)

    def piece(n, j, h, b=0):
        return tok.at[n, j, pl.ds(b * seqs + h * half, half)]

    def to_twin(n, key, j, h):
        remote(piece(n, j, h), piece(n, j, h, 1), twin, "twin", ("twin", n, key))

    def enter(n, h):
        if n:
            absorb(home_in.at[0, 0:half], arrival(("chips", n, h)))
        block = piece(n, t, h)
        if n in direct_in:
            remote(block, block, side_o, "relay", ("corner", n))
        remote(block, block, side_b, "side", ("side", n, h))
        remote(block, block, side_a, "side", ("side", n, h))
        to_twin(n, "tba", t, h)

    def relay(n, h):
        absorb(home_in.at[0:2, 0:half], arrival(("side", n, h)))
        if n not in direct_in:
            block, peer = (piece(n, beside, 0), side_a) if h == 0 else (piece(n, across, 1), side_b)
            remote(block, block, peer, "relay", ("corner", n))
        to_twin(n, "tba", beside, h)
        to_twin(n, "tba", across, h)

    def corner(n):
        absorb(home_in.at[0], arrival(("corner", n)))
        whole = tok.at[n, opposite, pl.ds(0, seqs)]
        remote(whole, tok.at[n, opposite, pl.ds(seqs, seqs)], twin, "twin", ("twin", n, "o"))

    def logits():
        stream_f = tok[0, t, 0:seqs].astype(f32)
        logit_all[t] = jnp.zeros(logit_all.shape[1:], f32)
        logit_all[t, 0:ep, 0:seqs] = lax.dot_general(
            router_ref[:, pl.ds(pl.multiple_of(t * cols, cols), cols)],
            stream_f * gains[1, t],
            last,
            precision=lax.Precision.HIGHEST,
            preferred_element_type=f32,
        )
        energy = jnp.sum(stream_f * stream_f, axis=1, keepdims=True)
        logit_all[t, ep : ep + 1, 0:seqs] = jnp.sum(
            jnp.where(row_i == col_i, energy, 0.0), axis=0, keepdims=True
        )
        gather(logit_all.at[t], logit_all.at[t], "g3", "g3")

    def weights():
        absorb(logit_all.at[0 : tp - 1], arrival("g3"))
        whole = logit_all[0]
        for j in range(1, tp):
            whole = whole + logit_all[j]
        whole = whole[:, 0:seqs]
        inverse = lax.rsqrt(whole[ep : ep + 1] / width + EPSILON)
        chosen = routed_t > 0.5
        expon = jnp.where(chosen, jnp.exp(jnp.where(chosen, whole[0:ep] * inverse, 0.0)), 0.0)
        weight_all[0] = jnp.zeros(weight_all.shape[1:], f32)
        weight_all[0, 0:ep, 0:seqs] = expon / jnp.sum(expon, axis=0, keepdims=True)
        weight_all[0, ep : ep + 1, 0:seqs] = inverse
        for k in range(1, ep):
            remote(weight_all.at[0], weight_all.at[k], (flip(me, k), t), "weight", "weight")

    def scale_in(n, key):
        places = {"tba": [t, beside, across], "o": [opposite]}[key]
        absorb(res_all.at[0 : len(places)], arrival(("twin", n, key)))
        for j in places:
            span = pl.ds(pl.multiple_of(j * cols, cols), cols)
            ready[n, :, span] = (tok[n, j].astype(f32) * gains[1, j]).astype(bf16)

    def column(line):
        return jnp.sum(jnp.where(row_i == col_i, line, 0.0), axis=1, keepdims=True)

    def expert(n):
        if n == outs[0]:
            loaded("experts")
            absorb(weight_all.at[0 : ep - 1], arrival("weight"))
        norm, share = [], []
        for b in range(2):
            norm.append(column(weight_all[2 * n + b, ep : ep + 1, 0:seqs]))
            share.append(column(weight_all[2 * n + b, pl.ds(me, 1), 0:seqs]))
        norm, share = jnp.concatenate(norm, axis=0), jnp.concatenate(share, axis=0)
        for c in range(0, hidden, piece_cols):
            gate_pre = dot(ready[n], wgu[:, c : c + piece_cols])
            up_pre = dot(ready[n], wgu[:, hidden + c : hidden + c + piece_cols])
            gate_cl = jnp.minimum(gate_pre * norm, LIMIT)
            up_cl = jnp.clip(up_pre * norm, -LIMIT, LIMIT)
            value = ((up_cl + 1.0) * share) * (gate_cl * jax.nn.sigmoid(ALPHA * gate_cl))
            act[n, :, c : c + piece_cols] = value.astype(bf16)

    def expert_out(n):
        if n == outs[0]:
            loaded("down")
        for number, j in enumerate((opposite, beside, across, t)):
            value = dot(act[n], wd[j])
            sib_out[n, j] = value[seqs:].astype(bf16)
            mine[n, j] = value[:seqs]
            if number == 0 and n in early_out:
                remote(sib_out.at[n, j], sib_in.at[n, j], twin, "back", ("corner back", n))
        if n in early_out:
            for j in (beside, across, t):
                remote(sib_out.at[n, j], sib_in.at[n, j], twin, "back", ("back", n))
        else:
            remote(sib_out.at[n], sib_in.at[n], twin, "back", ("back", n))

    def add_twin(n, j):
        both = mine[n, j] + sib_in[n, j].astype(f32)
        mine[n, j] = both
        summed[n, j] = both.astype(bf16)

    def cut(n, p, side=0):
        size = half // (2 if n in split_out else 1)
        return pl.ds(side * half + p * size, size)

    def parts(n):
        return range(2 if n in split_out else 1)

    def reduce_corner(n):
        if n in early_out:
            absorb(sib_in.at[n, 0], arrival(("corner back", n)))
        else:
            absorb(sib_in.at[n], arrival(("back", n)))
        add_twin(n, opposite)
        for p in parts(n):
            for side, peer in ((0, side_b), (1, side_a)):
                block = summed.at[n, opposite, cut(n, p, side)]
                remote(block, fwd_in.at[n, side, cut(n, p)], peer, "sum", ("fwd", n, p))

    def reduce_sides(n):
        if n in early_out:
            absorb(sib_in.at[n, 0 : tp - 1], arrival(("back", n)))
        add_twin(n, beside)
        add_twin(n, across)
        for p in parts(n):
            for side, peer, j in ((0, side_b, beside), (1, side_a, across)):
                block = summed.at[n, j, cut(n, p, side)]
                remote(block, from_side.at[n, side, cut(n, p, side)], peer, "sum", ("mine", n, p))

    def reduce_chip(n):
        reduce_corner(n)
        reduce_sides(n)

    def reduce_relay(n, p=0):
        here = cut(n, p)
        absorb(fwd_in.at[n, :, here], arrival(("fwd", n, p)))
        for side, peer, j in ((0, side_a, across), (1, side_b, beside)):
            there = cut(n, p, side)
            fwd_out[n, side, here] = (mine[n, j, there] + fwd_in[n, side, here].astype(f32)).astype(bf16)
            remote(fwd_out.at[n, side, here], from_side.at[n, 1 - side, there], peer, "sum", ("mine", n, p))

    def go_home(n, p=0):
        size = half // len(parts(n))
        absorb(from_side.at[n, 0:2, 0 : 2 * size], arrival(("mine", n, p)))
        for side in range(2):
            there = cut(n, p, side)
            value = mine[n, t, there] + sib_in[n, t, there].astype(f32)
            value = value + from_side[n, 0, there].astype(f32) + from_side[n, 1, there].astype(f32)
            if n:
                home_out[n, there] = value.astype(bf16)
                remote(home_out.at[n, there], home_in.at[n, there], (flip(me, 2 * n), t), "home", "home")
            else:
                mine[n, t, there] = value

    def finish():
        result = tok[0, t, 0:seqs].astype(f32) + mine[0, t]
        absorb(home_in.at[0 : chips - 1], arrival("home"))
        for n in range(1, chips):
            result = result + home_in[n].astype(f32)
        out_ref[...] = result.astype(bf16)

    outs, early_out, split_out, direct_in = (0, 1, 2, 3), (3,), (), ()
    plan = [
        (begin, 0), (begin, 1), (gate, 0), (gate, 1), (project, 0), (project, 1), (logits,), (relay, 0, 0),
        (enter, 1, 0), (relay, 0, 1), (enter, 1, 1), (weights,), (enter, 2, 0), (enter, 2, 1), (relay, 1, 0),
        (corner, 0), (scale_in, 0, "tba"), (relay, 1, 1), (enter, 3, 0), (enter, 3, 1), (scale_in, 0, "o"),
        (expert, 0), (relay, 2, 0), (relay, 2, 1), (scale_in, 1, "tba"), (corner, 1), (expert_out, 0),
        (relay, 3, 0), (relay, 3, 1), (scale_in, 2, "tba"), (scale_in, 1, "o"), (expert, 1), (corner, 2),
        (reduce_chip, 0), (expert_out, 1), (corner, 3), (scale_in, 3, "tba"), (scale_in, 2, "o"), (expert, 2),
        (reduce_chip, 1), (expert_out, 2), (reduce_relay, 0), (scale_in, 3, "o"), (expert, 3), (reduce_chip, 2),
        (expert_out, 3), (reduce_relay, 1), (go_home, 0), (reduce_chip, 3), (reduce_relay, 2), (go_home, 1),
        (reduce_relay, 3), (go_home, 2), (go_home, 3), (finish,),
    ]
    for step in plan:
        step[0](*step[1:])
    block = seqs * cols
    sent = 3 * block + 6 * seqs * chans + (chips - 1) * 2 * block + chips * (2 + 1 + 4 + 4 + 3) * block
    absorb(wgu.at[0 : sent // (2 * hidden)], send_sem.at[SENDS.index("rows")])
    absorb(logit_all.at[0 : tp - 1], send_sem.at[SENDS.index("g3")])
    absorb(weight_all.at[0 : ep - 1], send_sem.at[SENDS.index("weight")])


def finish_kernel(a_in, b_in, c_in, a_out, b_out, c_out, sems):
    writes = [
        pltpu.make_async_copy(held, target, sems.at[n])
        for n, (held, target) in enumerate(((a_in, a_out), (b_in, b_out), (c_in, c_out)))
    ]
    for write in writes:
        write.start()
    for write in writes:
        write.wait()


def dispatch(*args):
    (
        residual, state_re, state_im, mix_gain, proj_in, decay_rate, frequency, log_step,
        input_re, input_im, read_re, read_im, skip_gain, glu_weight, out_proj, ffn_gain,
        router, gate_weight, up_weight, down_weight, route_ids,
    ) = args
    ep, tp = lax.axis_size("ep"), lax.axis_size("tp")
    seqs, cols = residual.shape
    groups, states = decay_rate.shape
    chans = skip_gain.shape[0]
    rough = groups % 16 or chans % 128 or cols % 128 or seqs % 32 or seqs > 128
    if gate_weight.shape[0] != 1 or tp != 4 or ep != 8 or rough:
        return per_device(*args)
    top = route_ids.shape[1]
    hidden = gate_weight.shape[2]
    width = mix_gain.shape[0]
    chips = ep // 2
    bf16, f32 = jnp.bfloat16, jnp.float32
    hbm, vmem = pl.BlockSpec(memory_space=pltpu.HBM), pl.BlockSpec(memory_space=pltpu.VMEM)
    state_shape = (seqs, groups, states)
    blocks = (chips, tp, seqs, cols)
    out = pl.pallas_call(
        functools.partial(layer_kernel, (ep, tp)),
        out_shape=(
            pltpu.VMEM((seqs, cols), bf16),
            pltpu.VMEM(state_shape, f32),
            pltpu.VMEM(state_shape, f32),
        ),
        in_specs=[hbm] * 21,
        out_specs=(vmem, vmem, vmem),
        scratch_shapes=[
            pltpu.VMEM((seqs, cols), bf16),
            pltpu.VMEM((2, tp, 1, cols), f32),
            pltpu.VMEM((2, groups, states), f32),
            pltpu.VMEM((1, groups), f32),
            pltpu.VMEM((2, groups, chans // groups, states), f32),
            pltpu.VMEM((2, chans, states), f32),
            pltpu.VMEM((1, chans), f32),
            pltpu.VMEM((ep, width), f32),
            pltpu.VMEM((top, seqs), jnp.int32),
            pltpu.VMEM((2,) + state_shape, f32),
            pltpu.VMEM(proj_in.shape, bf16),
            pltpu.VMEM(glu_weight.shape, bf16),
            pltpu.VMEM(out_proj.shape, bf16),
            pltpu.VMEM((width, 2 * hidden), bf16),
            pltpu.VMEM((tp, hidden, cols), bf16),
            pltpu.VMEM((tp, seqs, cols), bf16),
            pltpu.VMEM((tp, seqs, chans), bf16),
            pltpu.VMEM((tp, seqs, chans), bf16),
            pltpu.VMEM((tp, 2 * ep, 128), f32),
            pltpu.VMEM((ep, 2 * ep, 128), f32),
            pltpu.VMEM((chips, tp, 2 * seqs, cols), bf16),
            pltpu.VMEM((chips, 2 * seqs, width), bf16),
            pltpu.VMEM((chips, 2 * seqs, hidden), bf16),
            pltpu.VMEM(blocks, f32),
            pltpu.VMEM(blocks, bf16),
            pltpu.VMEM(blocks, bf16),
            pltpu.VMEM(blocks, bf16),
            pltpu.VMEM((chips, 3, seqs, cols), bf16),
            pltpu.VMEM((chips, 2, seqs // 2, cols), bf16),
            pltpu.VMEM((chips, 2, seqs // 2, cols), bf16),
            pltpu.VMEM((chips, seqs, cols), bf16),
            pltpu.VMEM((chips, seqs, cols), bf16),
            pltpu.SemaphoreType.DMA((15,)),
            pltpu.SemaphoreType.DMA((len(SENDS),)),
            pltpu.SemaphoreType.DMA((34,)),
        ],
        compiler_params=pltpu.CompilerParams(
            collective_id=0, has_side_effects=True, vmem_limit_bytes=48 * 1024 * 1024
        ),
        name="layer",
    )(*(pltpu.with_memory_space_constraint(part, pltpu.HBM) for part in (
        residual,
        mix_gain.reshape(tp, 1, cols),
        ffn_gain.reshape(tp, 1, cols),
        decay_rate,
        frequency,
        log_step.reshape(1, groups),
        input_re.transpose(0, 2, 1),
        input_im.transpose(0, 2, 1),
        read_re.reshape(chans, states),
        read_im.reshape(chans, states),
        skip_gain.reshape(1, chans),
        router.T,
        route_ids.T,
        state_re,
        state_im,
        proj_in,
        glu_weight,
        out_proj,
        gate_weight.reshape(gate_weight.shape[1:]),
        up_weight.reshape(up_weight.shape[1:]),
        down_weight.reshape(down_weight.shape[1:]),
    )))
    return pl.pallas_call(
        finish_kernel,
        out_shape=tuple(jax.ShapeDtypeStruct(part.shape, part.dtype) for part in out),
        in_specs=[vmem] * 3,
        out_specs=(hbm,) * 3,
        scratch_shapes=[pltpu.SemaphoreType.DMA((3,))],
        compiler_params=pltpu.CompilerParams(vmem_limit_bytes=8 * 1024 * 1024),
        name="finish",
    )(*out)


def solution(mesh):
    in_specs = (
        P("ep", "tp"),
        P("ep", "tp", None),
        P("ep", "tp", None),
        P(),
        P(None, "tp"),
        P("tp", None),
        P("tp", None),
        P("tp"),
        P("tp", None, None),
        P("tp", None, None),
        P("tp", None, None),
        P("tp", None, None),
        P("tp"),
        P(None, "tp"),
        P(None, "tp"),
        P(),
        P(),
        P("ep", None, "tp"),
        P("ep", None, "tp"),
        P("ep", "tp", None),
        P("ep", None),
    )
    out_specs = (P("ep", "tp"), P("ep", "tp", None), P("ep", "tp", None))
    return jax.shard_map(
        dispatch, mesh=mesh, in_specs=in_specs, out_specs=out_specs, check_vma=False
    )
```
